256 devices in a mesh: sp: 32 (over z, x), fs: 4 (over y), tp: 2 (over core).
Axes of the slice: x: 4, y: 4, z: 8, core: 2. Of those that a mesh axis runs over, the one named last changes fastest.
Arguments:
- tokens: bfloat16 [4, 6144, 2048], P('fs', 'sp', 'tp'), may hold values from -24 to 24
- norm_gain: bfloat16 [2048], P('tp'), may hold values from 0.099609375 to 1.8984375
- w_q_down: bfloat16 [2048, 512], P('fs'), may hold values from -0.151 to 0.151
- q_gain: float32 [512], replicated, may hold values from 0.1 to 1.9
- w_q_nope: bfloat16 [512, 2048], P(None, 'tp'), may hold values from -1.21 to 1.21
- w_q_rope: bfloat16 [512, 1024], P(None, 'tp'), may hold values from -0.75 to 0.75
- w_kv_down: bfloat16 [2048, 256], P('fs'), may hold values from -0.151 to 0.151
- kv_gain: float32 [256], replicated, may hold values from 0.1 to 1.9
- w_k_up: bfloat16 [256, 2048], P(None, 'tp'), may hold values from -0.81 to 0.81
- w_v_up: bfloat16 [256, 2048], P(None, 'tp'), may hold values from -0.375 to 0.375
- w_k_rope: bfloat16 [2048, 64], replicated, may hold values from -0.125 to 0.125
- w_pool_in: bfloat16 [2048, 1024], P(None, 'tp'), may hold values from -0.125 to 0.125
- w_pool_mix: bfloat16 [4, 256, 256], replicated, may hold values from -0.375 to 0.375
- w_out_attn: bfloat16 [2048, 2048], P('tp'), may hold values from -0.125 to 0.125
- w_out_pool: bfloat16 [1024, 2048], P('tp'), may hold values from -0.1875 to 0.1875
Outputs:
- mixed: bfloat16 [4, 6144, 2048], P('fs', ('sp', 'tp'))
The draws below stay inside these ranges and needn't reach their ends.
All inputs are finite; a program needn't handle non-finite values.
Results may differ from the reference program's by a relative error of at most 0.02.
Values may be sent and summed in bfloat16 or wider, within the bound.
A program may use at most 128 MiB of HBM per device.

```python
import jax
import jax.numpy as jnp
from jax import lax

D_MODEL = 2048
HEADS = 16
NOPE_DIM = 128
ROPE_DIM = 64
VALUE_DIM = 128
Q_RANK = 512
KV_RANK = 256
POOL_CH = 1024
GRID_W = 64
TOK_DEV = 192
POOL_GROUP = 256
SEQS = 4
SEQ_LEN = 6144


def draw_tokens(key, part):
    base = jax.random.normal(jax.random.fold_in(key, 11), (SEQS, SEQ_LEN, D_MODEL), jnp.float32)
    return jnp.clip(base, -6.0, 6.0).astype(jnp.bfloat16)


def draw_w_q_down(key, part):
    base = jax.random.normal(jax.random.fold_in(key, 21), (D_MODEL, Q_RANK), jnp.float32)
    base = jnp.clip(base, -6.0, 6.0) * D_MODEL ** (-0.5)
    return jnp.clip(base, -0.15, 0.15).astype(jnp.bfloat16)


def draw_w_kv_down(key, part):
    base = jax.random.normal(jax.random.fold_in(key, 31), (D_MODEL, KV_RANK), jnp.float32)
    base = jnp.clip(base, -6.0, 6.0) * D_MODEL ** (-0.5)
    return jnp.clip(base, -0.15, 0.15).astype(jnp.bfloat16)


def draw_w_q_nope(key, part):
    base = jax.random.normal(jax.random.fold_in(key, 41), (Q_RANK, HEADS * NOPE_DIM), jnp.float32)
    base = jnp.clip(base, -6.0, 6.0) * (Q_RANK // 9) ** (-0.5)
    return jnp.clip(base, -1.2, 1.2).astype(jnp.bfloat16)


def draw_w_k_up(key, part):
    base = jax.random.normal(jax.random.fold_in(key, 51), (KV_RANK, HEADS * NOPE_DIM), jnp.float32)
    base = jnp.clip(base, -6.0, 6.0) * KV_RANK ** (-0.5)
    return jnp.clip(base, -0.8, 0.8).astype(jnp.bfloat16)


def block_levels(rng, dims, cuts, least, high):
    def one(axis_at, parts):
        heights = jax.random.uniform(jax.random.fold_in(jax.random.fold_in(rng, 6), axis_at), (parts,), jnp.float32, least / len(cuts), high / len(cuts))
        return jnp.repeat(jnp.exp(heights), dims[axis_at] // parts).reshape((-1,) + (1,) * (len(dims) - axis_at - 1))

    level = one(*cuts[0])
    for cut in cuts[1:]:
        level = level * one(*cut)
    return level


def scatter_about(own_key, shape, scale, reach, cuts=(), kind=jnp.bfloat16):
    values = scale * jax.random.normal(own_key, shape, jnp.float32)
    if cuts:
        values = values * block_levels(own_key, shape, cuts, -0.22, 0.18)
    return jnp.clip(values, -reach, reach).astype(kind)


def setup_inputs(seed: int = 0) -> dict:
    arg_keys = jax.random.split(jax.random.key(seed), 16)
    return {
        "tokens": draw_tokens(jax.random.fold_in(arg_keys[15], 71), 0),
        "norm_gain": jnp.clip(1.0 + 0.18 * jax.random.normal(arg_keys[1], (D_MODEL,), jnp.float32), 0.099609375, 1.8984375).astype(jnp.bfloat16),
        "w_q_down": draw_w_q_down(jax.random.fold_in(arg_keys[15], 71), 0),
        "q_gain": jnp.clip(1.0 + 0.18 * jax.random.normal(arg_keys[3], (Q_RANK,), jnp.float32), 0.1, 1.9),
        "w_q_nope": draw_w_q_nope(jax.random.fold_in(arg_keys[15], 71), 0),
        "w_q_rope": scatter_about(arg_keys[5], (Q_RANK, HEADS * ROPE_DIM), (Q_RANK // 9) ** -0.5, 0.75, ((1, 2),)),
        "w_kv_down": draw_w_kv_down(jax.random.fold_in(arg_keys[15], 71), 0),
        "kv_gain": jnp.clip(1.0 + 0.18 * jax.random.normal(arg_keys[7], (KV_RANK,), jnp.float32), 0.1, 1.9),
        "w_k_up": draw_w_k_up(jax.random.fold_in(arg_keys[15], 71), 0),
        "w_v_up": scatter_about(arg_keys[9], (KV_RANK, HEADS * VALUE_DIM), KV_RANK ** -0.5, 0.375, ((1, 2),)),
        "w_k_rope": scatter_about(arg_keys[10], (D_MODEL, ROPE_DIM), D_MODEL ** -0.5, 0.125),
        "w_pool_in": scatter_about(arg_keys[11], (D_MODEL, POOL_CH), D_MODEL ** -0.5, 0.125, ((1, 2),)),
        "w_pool_mix": scatter_about(arg_keys[12], (4, POOL_GROUP, POOL_GROUP), POOL_GROUP ** -0.5, 0.375),
        "w_out_attn": scatter_about(arg_keys[13], (HEADS * VALUE_DIM, D_MODEL), (HEADS * VALUE_DIM) ** -0.5, 0.125, ((0, 2),)),
        "w_out_pool": scatter_about(arg_keys[14], (POOL_CH, D_MODEL), POOL_CH ** -0.5, 0.1875, ((0, 2),)),
    }


EPS = 1e-06
THETA = 10000.0
window_sizes = (2, 4, 8, 16)

def normed(values, gain_vec):
    widened = values.astype(jnp.float32)
    scaled = widened * lax.rsqrt(lax.optimization_barrier(jnp.mean(widened * widened, axis=-1, keepdims=True)) + EPS)
    return (scaled * gain_vec.astype(jnp.float32)).astype(jnp.bfloat16)

def angles(position):
    row_index = (position // GRID_W).astype(jnp.float32)
    column = (position % GRID_W).astype(jnp.float32)
    inverse = THETA ** (-jnp.arange(0, ROPE_DIM // 2, 2).astype(jnp.float32) / (ROPE_DIM // 2))
    return jnp.stack([row_index, column], axis=-1)[:, :, None] * inverse

def rotate(values, angle_table):
    full_shape = values.shape
    split_parts = values.astype(jnp.float32).reshape(full_shape[:-1] + (2, 2, ROPE_DIM // 4))
    front_half = split_parts[..., 0, :]
    back_half = split_parts[..., 1, :]
    cosine = jnp.cos(angle_table)
    sine_part = jnp.sin(angle_table)
    turned = jnp.stack([front_half * cosine - back_half * sine_part, front_half * sine_part + back_half * cosine], axis=-2)
    return turned.reshape(full_shape).astype(jnp.bfloat16)

def attend(query_nope, query_rope, key_nope, key_rope, values_all):
    length = query_nope.shape[0]
    key_wide = key_nope.astype(jnp.float32)
    rope_wide = key_rope.astype(jnp.float32)
    value_wide = values_all.astype(jnp.float32)
    score_scale = (NOPE_DIM + ROPE_DIM) ** (-0.5)

    def one_block(block):
        query_part, rope_part = block
        scores = jnp.einsum('qhd,khd->hqk', query_part.astype(jnp.float32), key_wide)
        scores = scores + jnp.einsum('qhr,kr->hqk', rope_part.astype(jnp.float32), rope_wide)
        scores = scores * score_scale
        row_max = lax.optimization_barrier(jnp.max(scores, axis=-1, keepdims=True))
        weights = jnp.exp(scores - row_max)
        row_total = lax.optimization_barrier(jnp.sum(weights, axis=-1))
        rounded = lax.optimization_barrier(weights.astype(jnp.bfloat16))
        summed = jnp.einsum('hqk,khd->qhd', rounded.astype(jnp.float32), value_wide)
        return (summed / jnp.transpose(row_total)[:, :, None]).astype(jnp.bfloat16)
    blocks = length // TOK_DEV
    query_blocks = query_nope.reshape(blocks, TOK_DEV, HEADS, NOPE_DIM)
    rope_blocks = query_rope.reshape(blocks, TOK_DEV, HEADS, ROPE_DIM)
    result = lax.map(one_block, (query_blocks, rope_blocks))
    return result.reshape(length, HEADS * VALUE_DIM)

def pooled_mix(pool_in, w_pool_mix):
    length = pool_in.shape[0]
    sums = jnp.pad(jnp.cumsum(pool_in.astype(jnp.float32), axis=0), ((1, 0), (0, 0)))
    position = jnp.arange(length, dtype=jnp.int32)
    outputs = []
    for group, window in enumerate(window_sizes):
        low_edge = jnp.clip(position - window // 2, 0, length)
        high_edge = jnp.clip(position + window - window // 2, 0, length)
        group_sums = sums[:, group * POOL_GROUP:(group + 1) * POOL_GROUP]
        window_mean = (group_sums[high_edge] - group_sums[low_edge]) / (high_edge - low_edge).astype(jnp.float32)[:, None]
        spread = window_mean.astype(jnp.bfloat16) - pool_in[:, group * POOL_GROUP:(group + 1) * POOL_GROUP]
        outputs.append(jnp.dot(spread, w_pool_mix[group], preferred_element_type=jnp.float32).astype(jnp.bfloat16))
    return jnp.concatenate(outputs, axis=1)

def reference(tokens, norm_gain, w_q_down, q_gain, w_q_nope, w_q_rope, w_kv_down, kv_gain, w_k_up, w_v_up, w_k_rope, w_pool_in, w_pool_mix, w_out_attn, w_out_pool):

    def one_sequence(token_rows):
        length = token_rows.shape[0]
        position = jnp.arange(length, dtype=jnp.int32)
        angle_table = angles(position)
        hidden = normed(token_rows, norm_gain)
        q_latent = normed(jnp.dot(hidden, w_q_down, preferred_element_type=jnp.float32).astype(jnp.bfloat16), q_gain)
        kv_latent = normed(jnp.dot(hidden, w_kv_down, preferred_element_type=jnp.float32).astype(jnp.bfloat16), kv_gain)
        query_nope = jnp.dot(q_latent, w_q_nope, preferred_element_type=jnp.float32).astype(jnp.bfloat16)
        query_nope = query_nope.reshape(length, HEADS, NOPE_DIM)
        query_pre = jnp.dot(q_latent, w_q_rope, preferred_element_type=jnp.float32).astype(jnp.bfloat16)
        query_rope = rotate(query_pre.reshape(length, HEADS, ROPE_DIM), angle_table[:, None])
        key_nope = jnp.dot(kv_latent, w_k_up, preferred_element_type=jnp.float32).astype(jnp.bfloat16)
        key_nope = key_nope.reshape(length, HEADS, NOPE_DIM)
        values_all = jnp.dot(kv_latent, w_v_up, preferred_element_type=jnp.float32).astype(jnp.bfloat16)
        values_all = values_all.reshape(length, HEADS, VALUE_DIM)
        key_pre = jnp.dot(hidden, w_k_rope, preferred_element_type=jnp.float32).astype(jnp.bfloat16)
        key_rope = rotate(key_pre, angle_table)
        attended = attend(query_nope, query_rope, key_nope, key_rope, values_all)
        pool_in = jnp.dot(hidden, w_pool_in, preferred_element_type=jnp.float32).astype(jnp.bfloat16)
        pooled = pooled_mix(pool_in, w_pool_mix)
        combined = jnp.dot(attended, w_out_attn, preferred_element_type=jnp.float32)
        combined = combined + jnp.dot(pooled, w_out_pool, preferred_element_type=jnp.float32)
        return combined.astype(jnp.bfloat16)
    return lax.map(one_sequence, tokens)
```

```python
import jax
import jax.numpy as jnp
from jax import lax
from jax.experimental import pallas as pl
from jax.experimental.pallas import tpu as pltpu
from jax.sharding import Mesh
from jax.sharding import PartitionSpec as P

NOPE_DIM = 128
ROPE_DIM = 64
VALUE_DIM = 128
GRID_W = 64
POOL_GROUP = 256
SP = ("sp_0", "sp_1")
SP_TP = ("sp_0", "sp_1", "tp")


EPS = 1e-06
THETA = 10000.0
window_sizes = (2, 4, 8, 16)
rim_width = 8
span_limit = 1024


def sent_together(arrays, axis, dim, along):
    both = jnp.concatenate(arrays, axis=along)
    out, at, outs = (lax.all_gather(both, axis, axis=dim, tiled=True), 0, [])
    for a in arrays:
        outs.append(lax.slice_in_dim(out, at, at + a.shape[along], axis=along))
        at += a.shape[along]
    return tuple(outs)


def gathered_by_axis(array, axes, dim):
    out = array
    for number in range(len(axes) - 1, -1, -1):
        out = lax.all_gather(out, axes[number], axis=dim, tiled=True)
    return out


def padded_2(array, sides, width):
    for axis, dim in sides:
        size, length = (lax.axis_size(axis), array.shape[dim])
        up = [(i, (i + 1) % size) for i in range(size - 1)]
        down = [(j, i) for i, j in up]
        last = lax.slice_in_dim(array, length - width, length, axis=dim)
        first = lax.slice_in_dim(array, 0, width, axis=dim)
        before = lax.ppermute(last, axis, up)
        after = lax.ppermute(first, axis, down)
        array = jnp.concatenate([before, array, after], axis=dim)
    return array


def split_up(array, dim, length):
    shape = array.shape
    tiles = array.reshape(*shape[:dim], length, shape[dim] // length, *shape[dim + 1 :])
    return jnp.moveaxis(tiles, dim, 0)


def summed_on_arrival(array, axis, dim):
    tiles = split_up(array, dim, lax.axis_size(axis))
    arrived = lax.all_to_all(tiles, axis, split_axis=0, concat_axis=0, tiled=True)
    return arrived.astype(jnp.float32).sum(axis=0)


def normed(values, gain_vec):
    widened = values.astype(jnp.float32)
    scaled = widened * lax.rsqrt(jnp.mean(widened * widened, axis=-1, keepdims=True) + EPS)
    return (scaled * gain_vec.astype(jnp.float32)).astype(jnp.bfloat16)


def angles(position):
    row_index = (position // GRID_W).astype(jnp.float32)
    column = (position % GRID_W).astype(jnp.float32)
    inverse = THETA ** (-jnp.arange(0, ROPE_DIM // 2, 2).astype(jnp.float32) / (ROPE_DIM // 2))
    return jnp.stack([row_index, column], axis=-1)[:, :, None] * inverse


def rotate(values, angle_table):
    full_shape = values.shape
    split_parts = values.astype(jnp.float32).reshape(full_shape[:-1] + (2, 2, ROPE_DIM // 4))
    front_half = split_parts[..., 0, :]
    back_half = split_parts[..., 1, :]
    cosine = jnp.cos(angle_table)
    sine_part = jnp.sin(angle_table)
    turned = jnp.stack(
        [front_half * cosine - back_half * sine_part, front_half * sine_part + back_half * cosine],
        axis=-2,
    )
    return turned.reshape(full_shape).astype(jnp.bfloat16)


LOG2E = 1.4426950408889634
KB = 512
MB = 768
ROWS = 32


def attention_body(q_ref, kv_ref, o_ref, s_scr, p_scr, acc, m_s, l_s):
    bf, f32 = jnp.bfloat16, jnp.float32
    chunks = q_ref.shape[0] // MB
    blocks = kv_ref.shape[0] // KB

    def scores(i, h):
        k = kv_ref[pl.ds(pl.multiple_of(i * KB, KB), KB), :]
        s_scr[h] = lax.dot_general(
            q_ref[h * MB : (h + 1) * MB, :],
            k,
            (((1,), (1,)), ((), ())),
            preferred_element_type=f32,
        )

    def softmax(h):
        for r in range(0, MB, ROWS):
            g = slice(h * MB + r, h * MB + r + ROWS)
            s = [s_scr[h, r : r + ROWS, j * 128 : (j + 1) * 128] for j in range(KB // 128)]
            m_old = m_s[g, :]
            top = s[0]
            for t in s[1:]:
                top = jnp.maximum(top, t)
            m_new = jnp.maximum(m_old, jnp.max(top, axis=1, keepdims=True))
            alpha = jnp.exp2(m_old - m_new)
            total = l_s[g, :] * alpha
            for j, t in enumerate(s):
                p = jnp.exp2(t - m_new)
                total = total + p
                p_scr[h, r : r + ROWS, j * 128 : (j + 1) * 128] = p.astype(bf)
            m_s[g, :] = m_new
            l_s[g, :] = total
            for j in range(2):
                c = slice(j * 128, (j + 1) * 128)
                acc[g, c] = acc[g, c] * alpha

    def product(i, h):
        g = slice(h * MB, (h + 1) * MB)
        v = kv_ref[pl.ds(pl.multiple_of(i * KB, KB), KB), :256]
        acc[g, :] = acc[g, :] + jnp.dot(p_scr[h], v, preferred_element_type=f32)

    m_s[...] = jnp.full(m_s.shape, -1e30, f32)
    l_s[...] = jnp.zeros(l_s.shape, f32)
    acc[...] = jnp.zeros(acc.shape, f32)
    p_scr[...] = jnp.zeros(p_scr.shape, bf)
    scores(0, 0)

    def step(i, c):
        for h in range(chunks):
            last = h == chunks - 1
            scores(jnp.minimum(i + 1, blocks - 1) if last else i, (h + 1) % chunks)
            softmax(h)
            product(jnp.maximum(i - 1, 0) if h == 0 else i, (h - 1) % chunks)
        return c

    lax.fori_loop(0, blocks, step, 0)
    product(blocks - 1, chunks - 1)
    for r in range(0, q_ref.shape[0], 128):
        g = slice(r, r + 128)
        inv = 1.0 / jnp.sum(l_s[g, :], axis=1, keepdims=True)
        o_ref[g, :] = (acc[g, :] * inv).astype(bf)


def attention(q, kv):
    rows = q.shape[0]
    f32 = jnp.float32
    return pl.pallas_call(
        attention_body,
        out_shape=jax.ShapeDtypeStruct((rows, 256), jnp.bfloat16),
        in_specs=[pl.BlockSpec(memory_space=pltpu.VMEM)] * 2,
        out_specs=pl.BlockSpec(memory_space=pltpu.VMEM),
        scratch_shapes=[
            pltpu.VMEM((rows // MB, MB, KB), f32),
            pltpu.VMEM((rows // MB, MB, KB), jnp.bfloat16),
            pltpu.VMEM((rows, 256), f32),
            pltpu.VMEM((rows, 128), f32),
            pltpu.VMEM((rows, 128), f32),
        ],
        compiler_params=pltpu.CompilerParams(vmem_limit_bytes=48 * 2**20),
    )(q, kv)


def on_device(
    tokens,
    norm_gain,
    w_q_down,
    q_gain,
    w_q_nope,
    w_q_rope,
    w_kv_down,
    kv_gain,
    w_k_up,
    w_v_up,
    w_k_rope,
    w_pool_in,
    w_pool_mix,
    w_out_attn,
    w_out_pool,
):
    gathered_rows, gathered_gain = (
        lax.all_gather(tokens, "tp", axis=2, tiled=True),
        lax.all_gather(norm_gain, "tp", axis=0, tiled=True),
    )
    token_rows = gathered_rows[0]
    local_rows = token_rows.shape[0]
    q_down, kv_down = sent_together((w_q_down, w_kv_down), "fs", 0, 1)
    heads_dev = w_q_nope.shape[1] // NOPE_DIM
    length = local_rows * lax.axis_size(SP)
    position = lax.axis_index(SP) * local_rows + jnp.arange(local_rows, dtype=jnp.int32)
    angle_table = angles(position)
    hidden = normed(token_rows, gathered_gain)
    q_latent = normed(
        jnp.dot(hidden, q_down, preferred_element_type=jnp.float32).astype(jnp.bfloat16), q_gain
    )
    kv_latent = normed(
        jnp.dot(hidden, kv_down, preferred_element_type=jnp.float32).astype(jnp.bfloat16), kv_gain
    )
    query_nope = jnp.dot(q_latent, w_q_nope, preferred_element_type=jnp.float32).astype(
        jnp.bfloat16
    )
    query_nope = query_nope.reshape(local_rows, heads_dev, NOPE_DIM)
    query_pre = jnp.dot(q_latent, w_q_rope, preferred_element_type=jnp.float32).astype(jnp.bfloat16)
    query_rope = rotate(query_pre.reshape(local_rows, heads_dev, ROPE_DIM), angle_table[:, None])
    key_pre = jnp.dot(hidden, w_k_rope, preferred_element_type=jnp.float32).astype(jnp.bfloat16)
    key_rope = rotate(key_pre, angle_table)
    score_scale = (NOPE_DIM + ROPE_DIM) ** (-0.5)

    q_abs = jnp.einsum(
        "thd,chd->htc",
        query_nope,
        w_k_up.reshape(-1, heads_dev, NOPE_DIM),
        preferred_element_type=jnp.float32,
    ) * (score_scale * LOG2E)
    q_rot = jnp.transpose(query_rope, (1, 0, 2)).astype(jnp.float32) * (score_scale * LOG2E)
    q_all = jnp.concatenate(
        [q_abs.astype(jnp.bfloat16), q_rot.astype(jnp.bfloat16), jnp.zeros_like(query_rope).transpose(1, 0, 2)],
        axis=2,
    ).reshape(heads_dev * local_rows, 384)
    kv_dev = jnp.concatenate([kv_latent, key_rope, jnp.zeros_like(key_rope)], axis=1)
    out_latent = attention(q_all, gathered_by_axis(kv_dev, SP, 0))
    attended = jnp.einsum(
        "htc,chd->thd",
        out_latent.reshape(heads_dev, local_rows, 256),
        w_v_up.reshape(-1, heads_dev, VALUE_DIM),
        preferred_element_type=jnp.float32,
    ).astype(jnp.bfloat16)
    attended = attended.reshape(local_rows, heads_dev * VALUE_DIM)
    pool_in = jnp.dot(hidden, w_pool_in, preferred_element_type=jnp.float32).astype(jnp.bfloat16)
    groups_dev = pool_in.shape[1] // POOL_GROUP
    group_id = lax.axis_index("tp") * groups_dev + jnp.arange(groups_dev, dtype=jnp.int32)
    window = jnp.zeros((groups_dev,), jnp.int32)
    for group_index, window_size in enumerate(window_sizes):
        window = window + jnp.where(group_id == group_index, window_size, 0).astype(jnp.int32)
    window = jnp.repeat(window, POOL_GROUP)
    before = window // 2
    window_after = window - before
    padded = padded_2(pool_in, ((SP, 0),), 8)
    padded_wide = padded.astype(jnp.float32)
    window_sum = jnp.zeros(pool_in.shape, jnp.float32)
    for offset in range(-rim_width, rim_width):
        inside = ((offset >= -before) & (offset < window_after)).astype(jnp.float32)
        window_sum = (
            window_sum + padded_wide[rim_width + offset : rim_width + offset + local_rows] * inside
        )
    low_edge = jnp.clip(position[:, None] - before[None, :], 0, length)
    high_edge = jnp.clip(position[:, None] + window_after[None, :], 0, length)
    window_mean = (window_sum / (high_edge - low_edge).astype(jnp.float32)).astype(jnp.bfloat16)
    spread = (window_mean - pool_in).reshape(local_rows, groups_dev, POOL_GROUP)
    mixing = lax.dynamic_slice_in_dim(w_pool_mix, lax.axis_index("tp") * groups_dev, groups_dev, 0)
    pooled = jnp.einsum("tgc,gce->tge", spread, mixing, preferred_element_type=jnp.float32).astype(
        jnp.bfloat16
    )
    pooled = pooled.reshape(local_rows, groups_dev * POOL_GROUP)
    out_share = summed_on_arrival(
        (
            jnp.dot(attended, w_out_attn, preferred_element_type=jnp.float32)
            + jnp.dot(pooled, w_out_pool, preferred_element_type=jnp.float32)
        ).astype(jnp.bfloat16),
        "tp",
        0,
    )
    return out_share.astype(jnp.bfloat16)[None]


def solution(mesh):
    torus = Mesh(
        mesh.devices.reshape(8, 4, mesh.shape["fs"], mesh.shape["tp"]), ("sp_0", "sp_1", "fs", "tp")
    )
    placed = (
        P("fs", SP, "tp"),
        P("tp"),
        P("fs", None),
        P(),
        P(None, "tp"),
        P(None, "tp"),
        P("fs", None),
        P(),
        P(None, "tp"),
        P(None, "tp"),
        P(),
        P(None, "tp"),
        P(),
        P("tp", None),
        P("tp", None),
    )
    return jax.shard_map(
        on_device, mesh=torus, in_specs=placed, out_specs=P("fs", SP_TP, None), check_vma=False
    )
```

```python
import functools

import jax
import jax.numpy as jnp
import numpy as np
from jax import lax
from jax.experimental import pallas as pl
from jax.experimental.pallas import tpu as pltpu
from jax.sharding import Mesh
from jax.sharding import PartitionSpec as P

NOPE_DIM = 128
ROPE_DIM = 64
VALUE_DIM = 128
GRID_W = 64
POOL_GROUP = 256
SP = ("sp_0", "sp_1")
SP_TP = ("sp_0", "sp_1", "tp")
EPS = 1e-06
THETA = 10000.0
LOG2E = 1.4426950408889634
MESH = pl.DeviceIdType.MESH

NZ, NX, NY = 8, 4, 4
TOK = 192
HALF = 96
D = 2048
HEADS = 8
QR, KR = 512, 256
WIDE = 384
UNIT = 384
ROWS = HEADS * TOK
MB = 768
SUB = 32
SEQ = NZ * NX * TOK
SCALE = (NOPE_DIM + ROPE_DIM) ** (-0.5) * LOG2E
f32, bf16 = jnp.float32, jnp.bfloat16


def rope_tables():
    inverse = (THETA ** (-np.arange(0, ROPE_DIM // 2, 2) / (ROPE_DIM // 2))).astype(np.float32)
    lane = np.arange(128)
    freq = inverse[lane % 16]
    by_row = (lane // 32) % 2 == 0
    sign = np.where((lane // 16) % 2 == 0, -1.0, 1.0)

    def table(count, keep):
        angle = (np.arange(count, dtype=np.float32)[:, None] * freq).astype(np.float64)
        cos = np.where(keep, np.cos(angle), 0.0)
        sin = np.where(keep, np.sin(angle) * sign, 0.0)
        return np.stack([cos, sin]).astype(np.float32)

    return table(SEQ // GRID_W, by_row), table(GRID_W, ~by_row)


def turned(values, cos, sin):
    lane = lax.broadcasted_iota(jnp.int32, values.shape, 1)
    ahead = pltpu.roll(values, 112, 1)
    behind = pltpu.roll(values, 16, 1)
    partner = jnp.where((lane // 16) % 2 == 0, ahead, behind)
    return values * cos + partner * sin


def scaled_rows(values, gain, width):
    mean = jnp.sum(values * values, axis=1, keepdims=True) * (1.0 / width)
    return values * lax.rsqrt(mean + EPS) * gain


def layer_body(
    tokens,
    norm_gain,
    w_q_down,
    q_gain,
    w_q_nope,
    w_q_rope,
    w_kv_down,
    kv_gain,
    w_k_up,
    w_v_up,
    w_k_rope,
    w_pool_in,
    w_pool_mix,
    w_out_attn,
    w_out_pool,
    row_table,
    col_table,
    out,
    tok,
    gains,
    hidden,
    wkv,
    wq,
    wkr,
    wpi,
    wqn,
    wqr,
    wku,
    wvu,
    mix,
    woa,
    wop,
    cos_s,
    sin_s,
    kv,
    q_all,
    q_lat,
    q_nope,
    pool_in,
    halo,
    pooled,
    out_sum,
    att,
    send_buf,
    recv_buf,
    s_scr,
    p_scr,
    acc,
    m_s,
    l_s,
    loc,
    tok_ss,
    tok_rs,
    w_ss,
    w_rs,
    ws_ss,
    ws_rs,
    p1_ss,
    p1_rs,
    ring_ss,
    ring_rs,
    sib_ss,
    sib_rs,
    halo_ss,
    halo_rs,
    out_ss,
    out_rs,
):
    z, x = lax.axis_index("sp_0"), lax.axis_index("sp_1")
    y, c = lax.axis_index("fs"), lax.axis_index("tp")
    sp = z * NX + x
    other = {"tp": 1 - c}
    y_up, y_down = {"fs": lax.rem(y + 1, NY)}, {"fs": lax.rem(y + NY - 1, NY)}
    z_up, z_down = {"sp_0": lax.rem(z + 1, NZ)}, {"sp_0": lax.rem(z + NZ - 1, NZ)}
    x_up, x_down = {"sp_1": lax.rem(x + 1, NX)}, {"sp_1": lax.rem(x + NX - 1, NX)}
    sp_next, sp_prev = lax.rem(sp + 1, NZ * NX), lax.rem(sp + NZ * NX - 1, NZ * NX)
    next_dev = {"sp_0": sp_next // NX, "sp_1": sp_next % NX}
    prev_dev = {"sp_0": sp_prev // NX, "sp_1": sp_prev % NX}

    def remote(src, dst, ssem, rsem, dev):
        return pltpu.make_async_remote_copy(
            src_ref=src, dst_ref=dst, send_sem=ssem, recv_sem=rsem, device_id=dev, device_id_type=MESH
        )

    def local(i, src, dst):
        return pltpu.make_async_copy(src, dst, loc.at[i])

    loads = [
        local(0, tokens, tok.at[c]),
        local(1, norm_gain, gains.at[c]),
        local(2, w_kv_down, wkv.at[pl.ds(y * 512, 512)]),
        local(3, w_k_rope, wkr),
        local(4, w_pool_in, wpi),
        local(5, w_q_down, wq.at[pl.ds(y * 512, 512)]),
        local(6, w_pool_mix.at[pl.ds(2 * c, 2)], mix),
        local(7, w_out_pool, wop),
        local(8, w_q_nope, wqn),
        local(9, w_q_rope, wqr),
        local(10, w_k_up, wku),
        local(11, w_v_up, wvu),
        local(12, w_out_attn, woa),
    ]
    for copy in loads:
        copy.start()

    barrier = pltpu.get_barrier_semaphore()
    partners = [other, y_up, y_down, next_dev, prev_dev]
    partners += [{"sp_0": lax.rem(z + i, NZ)} for i in range(1, NZ)]
    partners += [{"sp_1": lax.rem(x + i, NX)} for i in range(1, NX)]
    for dev in partners:
        pl.semaphore_signal(barrier, inc=1, device_id=dev, device_id_type=MESH)
    pl.semaphore_wait(barrier, len(partners))

    tok_copy = remote(tokens, tok.at[c], tok_ss.at[0], tok_rs.at[0], other)
    gain_copy = remote(norm_gain, gains.at[c], tok_ss.at[1], tok_rs.at[1], other)
    tok_copy.start()
    gain_copy.start()

    def shard_rows(of, part, count):
        return pl.ds(of * 512 + c * 256 + part * 128, count)

    y1, y2, y3 = lax.rem(y + 3, NY), lax.rem(y + 1, NY), lax.rem(y + 2, NY)

    def weight_copies(w, hbm, buf):
        own_a, own_b = hbm.at[pl.ds(c * 256, 128)], hbm.at[pl.ds(c * 256 + 128, 128)]
        dst_a, dst_b = buf.at[shard_rows(y, 0, 128)], buf.at[shard_rows(y, 1, 128)]
        low, high = buf.at[shard_rows(y1, 0, 128)], buf.at[shard_rows(y2, 1, 128)]
        ss, rs = w_ss.at[w], w_rs.at[w]
        return dict(
            up1=remote(own_a, dst_a, ss.at[0], rs.at[0], y_up),
            up2=remote(own_b, dst_b, ss.at[1], rs.at[1], y_up),
            dn1=remote(own_b, dst_b, ss.at[2], rs.at[2], y_down),
            dn2=remote(own_a, dst_a, ss.at[3], rs.at[3], y_down),
            upf=remote(low, low, ss.at[4], rs.at[4], y_up),
            dnf=remote(high, high, ss.at[5], rs.at[5], y_down),
        )

    def weight_arrivals(w, hbm, buf):
        ss, rs = w_ss.at[w], w_rs.at[w]

        def got(i, of, part):
            view = buf.at[shard_rows(of, part, 128)]
            return remote(view, view, ss.at[i], rs.at[i], y_up)

        return dict(
            up1=got(0, y1, 0), up2=got(1, y1, 1), dn1=got(2, y2, 1), dn2=got(3, y2, 0), upf=got(4, y3, 0), dnf=got(5, y3, 1)
        )

    def weight_sibling(w, buf):
        ss, rs = ws_ss.at[w], ws_rs.at[w]
        sends, gots = [], []
        for i, of in enumerate((y1, y2, y3)):
            mine = buf.at[pl.ds(of * 512 + c * 256, 256)]
            theirs = buf.at[pl.ds(of * 512 + (1 - c) * 256, 256)]
            sends.append(remote(mine, mine, ss.at[i], rs.at[i], other))
            gots.append(remote(theirs, theirs, ss.at[i], rs.at[i], other))
        return sends, gots

    kvs, kva = weight_copies(0, w_kv_down, wkv), weight_arrivals(0, w_kv_down, wkv)
    qs, qa = weight_copies(1, w_q_down, wq), weight_arrivals(1, w_q_down, wq)
    kv_sib, kv_sib_got = weight_sibling(0, wkv)
    q_sib, q_sib_got = weight_sibling(1, wq)
    for name in ("up1", "dn1", "up2", "dn2"):
        kvs[name].start()
    for name in ("up1", "dn1"):
        qs[name].start()

    for k in range(TOK // GRID_W):
        rows = slice(k * GRID_W, (k + 1) * GRID_W)
        at = 3 * sp + k
        cos_s[rows, :] = row_table[0, pl.ds(at, 1), :] + col_table[0]
        sin_s[rows, :] = row_table[1, pl.ds(at, 1), :] + col_table[1]

    loads[0].wait()
    loads[1].wait()
    remote(tok.at[1 - c], tok.at[1 - c], tok_ss.at[0], tok_rs.at[0], other).wait_recv()
    remote(gains.at[1 - c], gains.at[1 - c], tok_ss.at[1], tok_rs.at[1], other).wait_recv()
    g0, g1 = gains[0].astype(f32), gains[1].astype(f32)
    for r in range(0, TOK, 16):
        a0, a1 = tok[0, r : r + 16, :].astype(f32), tok[1, r : r + 16, :].astype(f32)
        total = jnp.sum(a0 * a0 + a1 * a1, axis=1, keepdims=True)
        inv = lax.rsqrt(total * (1.0 / D) + EPS)
        hidden[r : r + 16, :1024] = (a0 * inv * g0).astype(bf16)
        hidden[r : r + 16, 1024:] = (a1 * inv * g1).astype(bf16)

    kva["up1"].wait_recv()
    kvs["upf"].start()
    kva["dn1"].wait_recv()
    kvs["dnf"].start()
    for name in ("up2", "dn2"):
        qs[name].start()
    kva["up2"].wait_recv()
    kv_sib[0].start()
    kva["dn2"].wait_recv()
    kv_sib[1].start()

    mine = pl.ds(c * HALF, HALF)
    loads[3].wait()
    key_pre = jnp.dot(hidden[mine, :], wkr[...], preferred_element_type=f32)
    key_pre = jnp.concatenate([key_pre, key_pre], axis=1).astype(bf16).astype(f32)
    key_rope = turned(key_pre, cos_s[mine, :], sin_s[mine, :]).astype(bf16)

    kva["upf"].wait_recv()
    kva["dnf"].wait_recv()
    kv_sib[2].start()
    loads[2].wait()
    for got in kv_sib_got:
        got.wait_recv()
    kv_pre = jnp.dot(hidden[mine, :], wkv[...], preferred_element_type=f32).astype(bf16)
    own0 = (z * NX + x) * HALF
    own1 = SEQ // 2 + (x * NZ + z) * HALF
    own_rows = pl.ds(pl.multiple_of(jnp.where(c == 0, own0, own1), HALF), HALF)
    kv[own_rows, :KR] = scaled_rows(kv_pre.astype(f32), kv_gain[...], KR).astype(bf16)
    kv[own_rows, KR:] = key_rope

    def blk0(zz, xx):
        return kv.at[pl.ds((zz * NX + xx) * HALF, HALF)]

    def blk1(zz, xx):
        return kv.at[pl.ds(SEQ // 2 + (xx * NZ + zz) * HALF, HALF)]

    def first0(i):
        to = lax.rem(x + i, NX)
        return remote(blk0(z, x), blk0(z, x), p1_ss.at[i], p1_rs.at[i], {"sp_1": to})

    def first0_got(i):
        view = blk0(z, lax.rem(x + NX - i, NX))
        return remote(view, view, p1_ss.at[i], p1_rs.at[i], x_up)

    def first1(i):
        to = lax.rem(z + i, NZ)
        return remote(blk1(z, x), blk1(z, x), p1_ss.at[i], p1_rs.at[i], {"sp_0": to})

    def first1_got(i):
        view = blk1(lax.rem(z + NZ - i, NZ), x)
        return remote(view, view, p1_ss.at[i], p1_rs.at[i], z_up)

    @pl.when(c == 0)
    def _():
        for i in (1, 3, 2):
            first0(i).start()

    @pl.when(c == 1)
    def _():
        for i in (1, 7, 2, 6, 3, 5, 4):
            first1(i).start()

    loads[4].wait()
    pool_in[...] = jnp.dot(hidden[...], wpi[...], preferred_element_type=f32).astype(bf16)
    halo_next = remote(pool_in.at[pl.ds(TOK - 16, 16)], halo.at[pl.ds(0, 16)], halo_ss.at[0], halo_rs.at[0], next_dev)
    halo_prev = remote(pool_in.at[pl.ds(0, 16)], halo.at[pl.ds(16, 16)], halo_ss.at[1], halo_rs.at[1], prev_dev)
    halo_next.start()
    halo_prev.start()

    qa["up1"].wait_recv()
    qs["upf"].start()
    qa["dn1"].wait_recv()
    qs["dnf"].start()

    dz = (0, -1, 1, -2, 2, -3, 3, 4)
    dxh = ((0, 0), (0, 1), (-1, 0), (1, 1), (-1, 1), (1, 0), (2, 0), (2, 1))

    def unit_row(cls, n):
        if cls == 0:
            return lax.rem(z + NZ + dz[n], NZ) * UNIT
        dx, h = dxh[n]
        return SEQ // 2 + lax.rem(x + NX + dx, NX) * 2 * UNIT + h * UNIT

    def unit(cls, n):
        return kv.at[pl.ds(unit_row(cls, n), UNIT)]

    def half_unit(n, h):
        return kv.at[pl.ds(unit_row(0, n) + h * (UNIT // 2), UNIT // 2)]

    def ring(src, i, dev):
        return remote(src, src, ring_ss.at[i], ring_rs.at[i], dev)

    def sends_after(cls, n):
        if cls == 0:
            if n == 0:
                return [ring(unit(0, 0), 1, z_up), ring(unit(0, 0), 2, z_down)]
            if n < 5:
                return [ring(unit(0, n), n + 2, z_up if n % 2 else z_down)]
            if n < 7:
                return [ring(half_unit(n, n - 5), n + 2, z_up if n % 2 else z_down)]
            return []
        if n == 0:
            return [
                ring(unit(1, 0), 1, x_up),
                ring(unit(1, 1), 2, x_down),
                ring(unit(1, 1), 3, x_up),
                ring(unit(1, 0), 4, x_down),
            ]
        if n == 2:
            return [ring(unit(1, 2), 5, x_up)]
        if n == 3:
            return [ring(unit(1, 3), 6, x_down)]
        return []

    def arrivals_for(cls, n):
        if cls == 0:
            if n == 7:
                return [ring(half_unit(7, 0), 7, z_up), ring(half_unit(7, 1), 8, z_up)]
            return [ring(unit(0, n), n, z_up)]
        return [ring(unit(1, n), n - 1, x_up)]

    def sib(cls, n):
        return remote(unit(cls, n), unit(cls, n), sib_ss.at[n], sib_rs.at[n], other)

    @pl.when(c == 0)
    def _():
        for i in (1, 3, 2):
            first0_got(i).wait_recv()
        for copy in sends_after(0, 0):
            copy.start()
        sib(0, 0).start()

    @pl.when(c == 1)
    def _():
        for i in (1, 7, 2, 6, 3, 5, 4):
            first1_got(i).wait_recv()
        for copy in sends_after(1, 0):
            copy.start()
        sib(1, 0).start()
        sib(1, 1).start()

    qa["up2"].wait_recv()
    q_sib[0].start()
    qa["dn2"].wait_recv()
    q_sib[1].start()

    remote(halo.at[pl.ds(0, 16)], halo.at[pl.ds(0, 16)], halo_ss.at[0], halo_rs.at[0], next_dev).wait_recv()
    remote(halo.at[pl.ds(16, 16)], halo.at[pl.ds(16, 16)], halo_ss.at[1], halo_rs.at[1], next_dev).wait_recv()
    loads[6].wait()
    loads[7].wait()
    row_i = lax.broadcasted_iota(jnp.int32, (TOK, TOK), 0)
    gap = lax.broadcasted_iota(jnp.int32, (TOK, TOK), 1) - row_i
    rim_row = lax.broadcasted_iota(jnp.int32, (TOK, 32), 0)
    rim_col = lax.broadcasted_iota(jnp.int32, (TOK, 32), 1)
    before = rim_col < 16
    rim_gap = jnp.where(before, rim_col - 16, rim_col - 16 + TOK) - rim_row
    rim_ok = (before & (sp > 0)) | (~before & (sp < NZ * NX - 1))
    place = lax.broadcasted_iota(jnp.int32, (TOK, POOL_GROUP), 0) + sp * TOK
    for g in range(2):
        span = (1 + 3 * c) * (1 + g)
        cols = slice(g * POOL_GROUP, (g + 1) * POOL_GROUP)
        near = ((gap >= -span) & (gap < span)).astype(f32).astype(bf16)
        rim = ((rim_gap >= -span) & (rim_gap < span) & rim_ok).astype(f32).astype(bf16)
        sums = jnp.dot(near, pool_in[:, cols], preferred_element_type=f32)
        sums = sums + jnp.dot(rim, halo[:, cols], preferred_element_type=f32)
        low = jnp.maximum(place - span, 0)
        high = jnp.minimum(place + span, SEQ)
        mean = (sums / (high - low).astype(f32)).astype(bf16)
        spread = (mean.astype(f32) - pool_in[:, cols].astype(f32)).astype(bf16)
        pooled[:, cols] = jnp.dot(spread, mix[g], preferred_element_type=f32).astype(bf16)
    for j in range(4):
        cols = slice(j * 512, (j + 1) * 512)
        out_sum[:, cols] = jnp.dot(pooled[...], wop[:, cols], preferred_element_type=f32)

    qa["upf"].wait_recv()
    qa["dnf"].wait_recv()
    q_sib[2].start()
    loads[5].wait()
    for i in (8, 9, 10):
        loads[i].wait()
    for got in q_sib_got:
        got.wait_recv()
    q_pre = jnp.dot(hidden[...], wq[...], preferred_element_type=f32).astype(bf16)
    q_lat[...] = scaled_rows(q_pre.astype(f32), q_gain[...], QR).astype(bf16)
    q_nope[...] = jnp.dot(q_lat[...], wqn[...], preferred_element_type=f32).astype(bf16)
    q_rot = jnp.dot(q_lat[...], wqr[...], preferred_element_type=f32).astype(bf16).astype(f32)
    lane = lax.broadcasted_iota(jnp.int32, (TOK, 128), 1)
    for h in range(HEADS):
        rows = slice(h * TOK, (h + 1) * TOK)
        if h % 2 == 0:
            pair = turned(q_rot[:, h * 64 : h * 64 + 128], cos_s[...], sin_s[...]) * SCALE
        keep = lane < 64 if h % 2 == 0 else lane >= 64
        q_all[rows, KR:] = jnp.where(keep, pair, 0.0).astype(bf16)
        head = slice(h * NOPE_DIM, (h + 1) * NOPE_DIM)
        absorbed = lax.dot_general(
            q_nope[:, head], wku[:, head], (((1,), (1,)), ((), ())), preferred_element_type=f32
        )
        q_all[rows, :KR] = (absorbed * SCALE).astype(bf16)

    last = 15

    def row_of(i):
        own = (i == 0) | ((lax.rem(i, 2) == 1) & (i < last))
        n = jnp.where(i == 0, 0, jnp.where(i == last, 7, jnp.where(own, (i + 1) // 2, i // 2 - 1)))
        cls = jnp.where(own, c, 1 - c)
        dzn = jnp.where(n == 7, 4, jnp.where(lax.rem(n, 2) == 1, -((n + 1) // 2), (n + 1) // 2))
        row0 = lax.rem(z + NZ + dzn, NZ) * UNIT
        dxn = jnp.where(n < 2, 0, jnp.where(n > 5, 2, jnp.where(lax.rem(n, 2) == 0, -1, 1)))
        hn = jnp.where(
            (n == 1) | (n == 3) | (n == 4) | (n == 7), 1, 0
        )
        row1 = SEQ // 2 + lax.rem(x + NX + dxn, NX) * 2 * UNIT + hn * UNIT
        return pl.multiple_of(jnp.where(cls == 0, row0, row1), UNIT), own, n

    def acquire(i):
        for n in range(1, 8):

            @pl.when((i == 2 * n - 1) & (c == 0))
            def _():
                for copy in arrivals_for(0, n):
                    copy.wait_recv()
                for copy in sends_after(0, n):
                    copy.start()
                sib(0, n).start()

            if n >= 2:

                @pl.when((i == 2 * n - 1) & (c == 1))
                def _():
                    for copy in arrivals_for(1, n):
                        copy.wait_recv()
                    for copy in sends_after(1, n):
                        copy.start()
                    sib(1, n).start()

        at, own, n = row_of(i)

        @pl.when(jnp.logical_not(own))
        def _():
            view = kv.at[pl.ds(at, UNIT)]
            remote(view, view, sib_ss.at[n], sib_rs.at[n], other).wait_recv()

        return at

    def scores(at, h):
        s_scr[h] = lax.dot_general(
            q_all[h * MB : (h + 1) * MB, :], kv[pl.ds(at, UNIT), :], (((1,), (1,)), ((), ())), preferred_element_type=f32
        )

    def softmax(h):
        for r in range(0, MB, SUB):
            g = slice(h * MB + r, h * MB + r + SUB)
            s = [s_scr[h, r : r + SUB, j * 128 : (j + 1) * 128] for j in range(UNIT // 128)]
            m_old = m_s[g, :]
            top = s[0]
            for t in s[1:]:
                top = jnp.maximum(top, t)
            m_new = jnp.maximum(m_old, jnp.max(top, axis=1, keepdims=True))
            alpha = jnp.exp2(m_old - m_new)
            total = l_s[g, :] * alpha
            for j, t in enumerate(s):
                p = jnp.exp2(t - m_new)
                total = total + p
                p_scr[h, r : r + SUB, j * 128 : (j + 1) * 128] = p.astype(bf16)
            m_s[g, :] = m_new
            l_s[g, :] = total
            for j in range(2):
                cols = slice(j * 128, (j + 1) * 128)
                acc[g, cols] = acc[g, cols] * alpha

    def product(at, h):
        g = slice(h * MB, (h + 1) * MB)
        acc[g, :] = acc[g, :] + jnp.dot(p_scr[h], kv[pl.ds(at, UNIT), :KR], preferred_element_type=f32)

    m_s[...] = jnp.full(m_s.shape, -1e30, f32)
    l_s[...] = jnp.zeros(l_s.shape, f32)
    acc[...] = jnp.zeros(acc.shape, f32)
    p_scr[1] = jnp.zeros(p_scr.shape[1:], bf16)
    scores(row_of(jnp.int32(0))[0], 0)

    def step(i, carry):
        now = row_of(i)[0]
        past = row_of(jnp.maximum(i - 1, 0))[0]
        nxt = jnp.minimum(i + 1, last)

        @pl.when(i < last)
        def _():
            acquire(i + 1)

        scores(now, 1)
        softmax(0)
        product(past, 1)
        scores(row_of(nxt)[0], 0)
        softmax(1)
        product(now, 0)
        return carry

    lax.fori_loop(0, last + 1, step, 0)
    product(row_of(jnp.int32(last))[0], 1)

    loads[11].wait()
    loads[12].wait()
    for h in range(HEADS):
        rows = slice(h * TOK, (h + 1) * TOK)
        head = slice(h * VALUE_DIM, (h + 1) * VALUE_DIM)
        total = jnp.sum(l_s[rows, :], axis=1, keepdims=True)
        weighted = (acc[rows, :] / total).astype(bf16)
        att[:, head] = jnp.dot(weighted, wvu[:, head], preferred_element_type=f32).astype(bf16)

    theirs = pl.ds((1 - c) * HALF, HALF)

    def share(j):
        return remote(send_buf.at[j], recv_buf.at[j], out_ss.at[j], out_rs.at[j], other)

    for j in range(4):
        cols = slice(j * 512, (j + 1) * 512)
        out_sum[:, cols] = out_sum[:, cols] + jnp.dot(att[...], woa[:, cols], preferred_element_type=f32)
        send_buf[j] = out_sum[theirs, cols].astype(bf16)
        share(j).start()
    for j in range(4):
        cols = slice(j * 512, (j + 1) * 512)
        share(j).wait_recv()
        out[:, cols] = (out_sum[mine, cols] + recv_buf[j].astype(f32)).astype(bf16)

    tok_copy.wait_send()
    gain_copy.wait_send()
    for group in (kvs, qs):
        for copy in group.values():
            copy.wait_send()
    for copy in kv_sib + q_sib:
        copy.wait_send()
    halo_next.wait_send()
    halo_prev.wait_send()
    for j in range(4):
        share(j).wait_send()

    @pl.when(c == 0)
    def _():
        for i in range(1, NX):
            first0(i).wait_send()
        for n in range(8):
            for copy in sends_after(0, n):
                copy.wait_send()
            sib(0, n).wait_send()

    @pl.when(c == 1)
    def _():
        for i in range(1, NZ):
            first1(i).wait_send()
        for n in range(8):
            for copy in sends_after(1, n):
                copy.wait_send()
            sib(1, n).wait_send()


def on_device(
    tokens,
    norm_gain,
    w_q_down,
    q_gain,
    w_q_nope,
    w_q_rope,
    w_kv_down,
    kv_gain,
    w_k_up,
    w_v_up,
    w_k_rope,
    w_pool_in,
    w_pool_mix,
    w_out_attn,
    w_out_pool,
):
    row_table, col_table = rope_tables()
    anywhere = pl.BlockSpec(memory_space=pl.ANY)
    vmem = pl.BlockSpec(memory_space=pltpu.VMEM)
    dma = pltpu.SemaphoreType.DMA
    result = pl.pallas_call(
        layer_body,
        out_shape=jax.ShapeDtypeStruct((HALF, D), bf16),
        in_specs=[anywhere, anywhere, anywhere, vmem, anywhere, anywhere, anywhere, vmem] + [anywhere] * 7 + [vmem, vmem],
        out_specs=vmem,
        scratch_shapes=[
            pltpu.VMEM((2, TOK, 1024), bf16),
            pltpu.VMEM((2, 1, 1024), bf16),
            pltpu.VMEM((TOK, D), bf16),
            pltpu.VMEM((D, KR), bf16),
            pltpu.VMEM((D, QR), bf16),
            pltpu.VMEM((D, ROPE_DIM), bf16),
            pltpu.VMEM((D, 512), bf16),
            pltpu.VMEM((QR, 1024), bf16),
            pltpu.VMEM((QR, 512), bf16),
            pltpu.VMEM((KR, 1024), bf16),
            pltpu.VMEM((KR, 1024), bf16),
            pltpu.VMEM((2, POOL_GROUP, POOL_GROUP), bf16),
            pltpu.VMEM((1024, D), bf16),
            pltpu.VMEM((512, D), bf16),
            pltpu.VMEM((TOK, 128), f32),
            pltpu.VMEM((TOK, 128), f32),
            pltpu.VMEM((SEQ, WIDE), bf16),
            pltpu.VMEM((ROWS, WIDE), bf16),
            pltpu.VMEM((TOK, QR), bf16),
            pltpu.VMEM((TOK, 1024), bf16),
            pltpu.VMEM((TOK, 512), bf16),
            pltpu.VMEM((32, 512), bf16),
            pltpu.VMEM((TOK, 512), bf16),
            pltpu.VMEM((TOK, D), f32),
            pltpu.VMEM((TOK, 1024), bf16),
            pltpu.VMEM((4, HALF, 512), bf16),
            pltpu.VMEM((4, HALF, 512), bf16),
            pltpu.VMEM((2, MB, UNIT), f32),
            pltpu.VMEM((2, MB, UNIT), bf16),
            pltpu.VMEM((ROWS, KR), f32),
            pltpu.VMEM((ROWS, 128), f32),
            pltpu.VMEM((ROWS, 128), f32),
            dma((13,)),
            dma((2,)),
            dma((2,)),
            dma((2, 6)),
            dma((2, 6)),
            dma((2, 3)),
            dma((2, 3)),
            dma((8,)),
            dma((8,)),
            dma((9,)),
            dma((9,)),
            dma((8,)),
            dma((8,)),
            dma((2,)),
            dma((2,)),
            dma((4,)),
            dma((4,)),
        ],
        compiler_params=pltpu.CompilerParams(
            collective_id=0, has_side_effects=True, vmem_limit_bytes=60 * 2**20
        ),
    )(
        tokens[0],
        norm_gain[None],
        w_q_down,
        q_gain[None],
        w_q_nope,
        w_q_rope,
        w_kv_down,
        kv_gain[None],
        w_k_up,
        w_v_up,
        w_k_rope,
        w_pool_in,
        w_pool_mix,
        w_out_attn,
        w_out_pool,
        jnp.asarray(row_table),
        jnp.asarray(col_table),
    )
    return result[None]


def solution(mesh):
    torus = Mesh(
        mesh.devices.reshape(NZ, NX, mesh.shape["fs"], mesh.shape["tp"]), ("sp_0", "sp_1", "fs", "tp")
    )
    placed = (
        P("fs", SP, "tp"),
        P("tp"),
        P("fs", None),
        P(),
        P(None, "tp"),
        P(None, "tp"),
        P("fs", None),
        P(),
        P(None, "tp"),
        P(None, "tp"),
        P(),
        P(None, "tp"),
        P(),
        P("tp", None),
        P("tp", None),
    )
    return jax.shard_map(
        on_device, mesh=torus, in_specs=placed, out_specs=P("fs", SP_TP, None), check_vma=False
    )
```

```python
import functools

import jax
import jax.numpy as jnp
import numpy as np
from jax import lax
from jax.experimental import pallas as pl
from jax.experimental.pallas import tpu as pltpu
from jax.sharding import Mesh
from jax.sharding import PartitionSpec as P

NOPE_DIM = 128
ROPE_DIM = 64
VALUE_DIM = 128
GRID_W = 64
POOL_GROUP = 256
SP = ("sp_0", "sp_1")
SP_TP = ("sp_0", "sp_1", "tp")
EPS = 1e-06
THETA = 10000.0
LOG2E = 1.4426950408889634
MESH = pl.DeviceIdType.MESH

NZ, NX, NY = 8, 4, 4
TOK = 192
HALF = 96
D = 2048
HEADS = 8
QR, KR = 512, 256
WIDE = 384
UNIT = 384
ROWS = HEADS * TOK
MB = 384
STEP = 2 * UNIT
SUB = 32
SEQ = NZ * NX * TOK
SCALE = (NOPE_DIM + ROPE_DIM) ** (-0.5) * LOG2E
f32, bf16 = jnp.float32, jnp.bfloat16


def rope_tables():
    inverse = (THETA ** (-np.arange(0, ROPE_DIM // 2, 2) / (ROPE_DIM // 2))).astype(np.float32)
    lane = np.arange(128)
    freq = inverse[lane % 16]
    by_row = (lane // 32) % 2 == 0
    sign = np.where((lane // 16) % 2 == 0, -1.0, 1.0)

    def table(count, keep):
        angle = (np.arange(count, dtype=np.float32)[:, None] * freq).astype(np.float64)
        cos = np.where(keep, np.cos(angle), 0.0)
        sin = np.where(keep, np.sin(angle) * sign, 0.0)
        return np.stack([cos, sin]).astype(np.float32)

    return table(SEQ // GRID_W, by_row), table(GRID_W, ~by_row)


def turned(values, cos, sin):
    lane = lax.broadcasted_iota(jnp.int32, values.shape, 1)
    ahead = pltpu.roll(values, 112, 1)
    behind = pltpu.roll(values, 16, 1)
    partner = jnp.where((lane // 16) % 2 == 0, ahead, behind)
    return values * cos + partner * sin


def scaled_rows(values, gain, width):
    mean = jnp.sum(values * values, axis=1, keepdims=True) * (1.0 / width)
    return values * lax.rsqrt(mean + EPS) * gain


def layer_body(
    tokens,
    norm_gain,
    w_q_down,
    q_gain,
    w_q_nope,
    w_q_rope,
    w_kv_down,
    kv_gain,
    w_k_up,
    w_v_up,
    w_k_rope,
    w_pool_in,
    w_pool_mix,
    w_out_attn,
    w_out_pool,
    row_hbm,
    col_hbm,
    out,
    tok,
    gains,
    q_gain_s,
    kv_gain_s,
    row_table,
    col_table,
    hidden,
    wkv,
    wq,
    wkr,
    wpi,
    wqn,
    wqr,
    wku,
    wvu,
    mix,
    woa,
    wop,
    cos_s,
    sin_s,
    kv,
    q_all,
    q_lat,
    q_nope,
    pool_in,
    halo,
    pooled,
    out_sum,
    att,
    send_buf,
    recv_buf,
    s_scr,
    p_scr,
    acc,
    m_s,
    l_s,
    loc,
    tok_ss,
    tok_rs,
    w_ss,
    w_rs,
    ws_ss,
    ws_rs,
    p1_ss,
    p1_rs,
    ring_ss,
    ring_rs,
    sib_ss,
    sib_rs,
    halo_ss,
    halo_rs,
    out_ss,
    out_rs,
):
    z, x = lax.axis_index("sp_0"), lax.axis_index("sp_1")
    y, c = lax.axis_index("fs"), lax.axis_index("tp")
    sp = z * NX + x
    other = {"tp": 1 - c}
    y_up, y_down = {"fs": lax.rem(y + 1, NY)}, {"fs": lax.rem(y + NY - 1, NY)}
    z_up, z_down = {"sp_0": lax.rem(z + 1, NZ)}, {"sp_0": lax.rem(z + NZ - 1, NZ)}
    x_up, x_down = {"sp_1": lax.rem(x + 1, NX)}, {"sp_1": lax.rem(x + NX - 1, NX)}
    sp_next, sp_prev = lax.rem(sp + 1, NZ * NX), lax.rem(sp + NZ * NX - 1, NZ * NX)
    next_dev = {"sp_0": sp_next // NX, "sp_1": sp_next % NX}
    prev_dev = {"sp_0": sp_prev // NX, "sp_1": sp_prev % NX}

    def remote(src, dst, ssem, rsem, dev):
        return pltpu.make_async_remote_copy(
            src_ref=src, dst_ref=dst, send_sem=ssem, recv_sem=rsem, device_id=dev, device_id_type=MESH
        )

    barrier = pltpu.get_barrier_semaphore()
    partners = [other, y_up, y_down, next_dev, prev_dev]
    partners += [{"sp_0": lax.rem(z + i, NZ)} for i in range(1, NZ)]
    partners += [{"sp_1": lax.rem(x + i, NX)} for i in range(1, NX)]
    for dev in partners:
        pl.semaphore_signal(barrier, inc=1, device_id=dev, device_id_type=MESH)

    def local(i, src, dst):
        return pltpu.make_async_copy(src, dst, loc.at[i])

    loads = [
        local(0, tokens, tok.at[c]),
        local(1, norm_gain, gains.at[c]),
        local(2, w_kv_down, wkv.at[pl.ds(y * 512, 512)]),
        local(3, w_k_rope, wkr),
        local(4, w_pool_in, wpi),
        local(5, w_q_down, wq.at[pl.ds(y * 512, 512)]),
        local(6, w_pool_mix.at[pl.ds(2 * c, 2)], mix),
        local(7, w_out_pool, wop),
        local(8, w_q_nope, wqn),
        local(9, w_q_rope, wqr),
        local(10, w_k_up, wku),
        local(11, w_v_up, wvu),
        local(12, w_out_attn, woa),
        local(13, q_gain, q_gain_s),
        local(14, kv_gain, kv_gain_s),
        local(15, row_hbm, row_table),
        local(16, col_hbm, col_table),
    ]
    for i in (0, 1, 2, 15, 16, 5):
        loads[i].start()

    m_s[...] = jnp.full(m_s.shape, -1e30, f32)
    l_s[...] = jnp.zeros(l_s.shape, f32)
    acc[...] = jnp.zeros(acc.shape, f32)
    pl.semaphore_wait(barrier, len(partners))

    tok_copy = remote(tok.at[c], tok.at[c], tok_ss.at[0], tok_rs.at[0], other)
    gain_copy = remote(gains.at[c], gains.at[c], tok_ss.at[1], tok_rs.at[1], other)
    loads[0].wait()
    loads[1].wait()
    tok_copy.start()
    gain_copy.start()

    y1, y2, y3 = lax.rem(y + 3, NY), lax.rem(y + 1, NY), lax.rem(y + 2, NY)

    def weight_copies(w, buf, base, part):
        def rows(of, p):
            return buf.at[pl.ds(of * 512 + base + p * part, part)]

        ss, rs = w_ss.at[w], w_rs.at[w]

        def copy(i, of, p, dev):
            return remote(rows(of, p), rows(of, p), ss.at[i], rs.at[i], dev)

        def sends(name):
            return {
                "up1": lambda: copy(0, y, 0, y_up),
                "up2": lambda: copy(1, y, 1, y_up),
                "dn1": lambda: copy(2, y, 1, y_down),
                "dn2": lambda: copy(3, y, 0, y_down),
                "upf": lambda: copy(4, y1, 0, y_up),
                "dnf": lambda: copy(5, y2, 1, y_down),
            }[name]()

        def got(name):
            return {
                "up1": lambda: copy(0, y1, 0, y_up),
                "up2": lambda: copy(1, y1, 1, y_up),
                "dn1": lambda: copy(2, y2, 1, y_up),
                "dn2": lambda: copy(3, y2, 0, y_up),
                "upf": lambda: copy(4, y3, 0, y_up),
                "dnf": lambda: copy(5, y3, 1, y_up),
            }[name]()

        return sends, got

    def weight_sibling(w, buf, base, count, i):
        view = buf.at[pl.ds((y1, y2, y3)[i] * 512 + base, count)]
        return remote(view, view, ws_ss.at[w, i], ws_rs.at[w, i], other)

    kv_send, kv_got = weight_copies(0, wkv, 0, 256)
    q_send, q_got = weight_copies(1, wq, c * 256, 128)

    def kv_sib(i):
        return weight_sibling(0, wkv, 0, 512, i)

    def q_sib(i):
        return weight_sibling(1, wq, c * 256, 256, i)

    def q_sib_got(i):
        return weight_sibling(1, wq, (1 - c) * 256, 256, i)

    def start_queries():
        for name in ("up1", "dn1", "up2", "dn2"):
            q_send(name).start()

    loads[2].wait()

    @pl.when(c == 1)
    def _():
        for name in ("up1", "dn1", "up2", "dn2"):
            kv_send(name).start()

    for i in (3, 4, 6, 7, 8, 9, 10, 11, 13, 14, 12):
        loads[i].start()
    loads[5].wait()

    loads[15].wait()
    loads[16].wait()
    for k in range(TOK // GRID_W):
        rows = slice(k * GRID_W, (k + 1) * GRID_W)
        at = 3 * sp + k
        cos_s[rows, :] = row_table[0, pl.ds(at, 1), :] + col_table[0]
        sin_s[rows, :] = row_table[1, pl.ds(at, 1), :] + col_table[1]

    remote(tok.at[1 - c], tok.at[1 - c], tok_ss.at[0], tok_rs.at[0], other).wait_recv()
    remote(gains.at[1 - c], gains.at[1 - c], tok_ss.at[1], tok_rs.at[1], other).wait_recv()
    gain = [gains[half].astype(f32) for half in range(2)]
    for r in range(0, TOK, 16):
        parts = [tok[half, r : r + 16, :].astype(f32) for half in range(2)]
        total = jnp.sum(parts[0] * parts[0] + parts[1] * parts[1], axis=1, keepdims=True)
        inv = lax.rsqrt(total * (1.0 / D) + EPS)
        for half in range(2):
            for j in range(8):
                cols = slice(j * 128, (j + 1) * 128)
                at = half * 1024 + j * 128
                hidden[r : r + 16, at : at + 128] = (parts[half][:, cols] * inv * gain[half][j : j + 1, :]).astype(bf16)
    @pl.when(c == 1)
    def _():
        kv_got("up1").wait_recv()
        kv_send("upf").start()
        kv_got("dn1").wait_recv()
        kv_send("dnf").start()
        start_queries()
        kv_got("up2").wait_recv()
        kv_sib(0).start()
        kv_got("dn2").wait_recv()
        kv_sib(1).start()

    @pl.when(c == 0)
    def _():
        kv_sib(0).wait_recv()
        start_queries()
        kv_sib(1).wait_recv()

    loads[4].wait()
    pool_in[...] = jnp.dot(hidden[...], wpi[...], preferred_element_type=f32).astype(bf16)
    halo_next = remote(pool_in.at[pl.ds(TOK - 16, 16)], halo.at[pl.ds(0, 16)], halo_ss.at[0], halo_rs.at[0], next_dev)
    halo_prev = remote(pool_in.at[pl.ds(0, 16)], halo.at[pl.ds(16, 16)], halo_ss.at[1], halo_rs.at[1], prev_dev)
    halo_next.start()
    halo_prev.start()

    mine = pl.ds(c * HALF, HALF)
    loads[3].wait()
    key_pre = lax.dot_general(
        hidden[mine, :], wkr[...], (((1,), (1,)), ((), ())), preferred_element_type=f32
    )
    key_pre = jnp.concatenate([key_pre, key_pre], axis=1).astype(bf16).astype(f32)
    key_rope = turned(key_pre, cos_s[mine, :], sin_s[mine, :]).astype(bf16)

    @pl.when(c == 1)
    def _():
        kv_got("upf").wait_recv()
        kv_got("dnf").wait_recv()
        kv_sib(2).start()

    @pl.when(c == 0)
    def _():
        kv_sib(2).wait_recv()

    loads[14].wait()
    kv_pre = jnp.dot(hidden[mine, :], wkv[...], preferred_element_type=f32).astype(bf16)
    own0 = x * HALF
    own1 = SEQ // 2 + z * HALF
    own_rows = pl.ds(pl.multiple_of(jnp.where(c == 0, own0, own1), HALF), HALF)
    kv[own_rows, :KR] = scaled_rows(kv_pre.astype(f32), kv_gain_s[...], KR).astype(bf16)
    kv[own_rows, KR:] = key_rope

    def blk0(xx):
        return kv.at[pl.ds(xx * HALF, HALF)]

    def blk1(zz):
        return kv.at[pl.ds(SEQ // 2 + zz * HALF, HALF)]

    def first0(i):
        to = lax.rem(x + i, NX)
        return remote(blk0(x), blk0(x), p1_ss.at[i], p1_rs.at[i], {"sp_1": to})

    def first0_got(i):
        view = blk0(lax.rem(x + NX - i, NX))
        return remote(view, view, p1_ss.at[i], p1_rs.at[i], x_up)

    def first1(i):
        to = lax.rem(z + i, NZ)
        return remote(blk1(z), blk1(z), p1_ss.at[i], p1_rs.at[i], {"sp_0": to})

    def first1_got(i):
        view = blk1(lax.rem(z + NZ - i, NZ))
        return remote(view, view, p1_ss.at[i], p1_rs.at[i], z_up)

    @pl.when(c == 0)
    def _():
        for i in (1, 3, 2):
            first0(i).start()

    @pl.when(c == 1)
    def _():
        for i in (1, 7, 2, 6, 3, 5, 4):
            first1(i).start()

    q_got("up1").wait_recv()
    q_send("upf").start()
    q_got("dn1").wait_recv()
    q_send("dnf").start()

    def unit(cls, n):
        return kv.at[pl.ds(cls * (SEQ // 2) + n * UNIT, UNIT)]

    def half_unit(n, h):
        return kv.at[pl.ds(n * UNIT + h * (UNIT // 2), UNIT // 2)]

    def ring(src, dst, i, dev):
        return remote(src, dst, ring_ss.at[i], ring_rs.at[i], dev)

    def sends_after(cls, n):
        if cls == 0:
            up, down = z_up, z_down
            if n == 0:
                return [ring(unit(0, 0), unit(0, 1), 1, up), ring(unit(0, 0), unit(0, 2), 2, down)]
            if n < 5:
                return [ring(unit(0, n), unit(0, n + 2), n + 2, up if n % 2 else down)]
            if n < 7:
                return [ring(half_unit(n, n - 5), half_unit(7, n - 5), n + 2, up if n % 2 else down)]
            return []
        up, down = x_up, x_down
        if n == 0:
            return [
                ring(unit(1, 0), unit(1, 2), 2, up),
                ring(unit(1, 1), unit(1, 3), 3, down),
                ring(unit(1, 1), unit(1, 4), 4, up),
                ring(unit(1, 0), unit(1, 5), 5, down),
            ]
        if n == 2:
            return [ring(unit(1, 2), unit(1, 6), 6, up)]
        if n == 3:
            return [ring(unit(1, 3), unit(1, 7), 7, down)]
        return []

    def arrivals_for(cls, n):
        if cls == 0 and n == 7:
            return [ring(half_unit(7, h), half_unit(7, h), 7 + h, z_up) for h in range(2)]
        return [ring(unit(cls, n), unit(cls, n), n, z_up)]

    def sib(cls, n):
        return remote(unit(cls, n), unit(cls, n), sib_ss.at[n], sib_rs.at[n], other)

    def acquire_own(cls, n):
        for copy in arrivals_for(cls, n):
            copy.wait_recv()
        for copy in sends_after(cls, n):
            copy.start()
        sib(cls, n).start()

    q_got("up2").wait_recv()
    q_sib(0).start()
    q_got("dn2").wait_recv()
    q_sib(1).start()

    @pl.when(c == 0)
    def _():
        for i in (1, 3, 2):
            first0_got(i).wait_recv()
        for copy in sends_after(0, 0):
            copy.start()
        sib(0, 0).start()


    remote(halo.at[pl.ds(0, 16)], halo.at[pl.ds(0, 16)], halo_ss.at[0], halo_rs.at[0], next_dev).wait_recv()
    remote(halo.at[pl.ds(16, 16)], halo.at[pl.ds(16, 16)], halo_ss.at[1], halo_rs.at[1], next_dev).wait_recv()
    loads[6].wait()
    loads[7].wait()
    row_i = lax.broadcasted_iota(jnp.int32, (TOK, TOK), 0)
    gap = lax.broadcasted_iota(jnp.int32, (TOK, TOK), 1) - row_i
    rim_row = lax.broadcasted_iota(jnp.int32, (TOK, 32), 0)
    rim_col = lax.broadcasted_iota(jnp.int32, (TOK, 32), 1)
    before = rim_col < 16
    rim_gap = jnp.where(before, rim_col - 16, rim_col - 16 + TOK) - rim_row
    rim_ok = (before & (sp > 0)) | (~before & (sp < NZ * NX - 1))
    place = lax.broadcasted_iota(jnp.int32, (TOK, POOL_GROUP), 0) + sp * TOK
    for g in range(2):
        span = (1 + 3 * c) * (1 + g)
        cols = slice(g * POOL_GROUP, (g + 1) * POOL_GROUP)
        near = ((gap >= -span) & (gap < span)).astype(f32).astype(bf16)
        rim = ((rim_gap >= -span) & (rim_gap < span) & rim_ok).astype(f32).astype(bf16)
        sums = jnp.dot(near, pool_in[:, cols], preferred_element_type=f32)
        sums = sums + jnp.dot(rim, halo[:, cols], preferred_element_type=f32)
        low = jnp.maximum(place - span, 0)
        high = jnp.minimum(place + span, SEQ)
        mean = (sums / (high - low).astype(f32)).astype(bf16)
        spread = (mean.astype(f32) - pool_in[:, cols].astype(f32)).astype(bf16)
        pooled[:, cols] = jnp.dot(spread, mix[g], preferred_element_type=f32).astype(bf16)
    for j in range(4):
        cols = slice(j * 512, (j + 1) * 512)
        out_sum[:, cols] = jnp.dot(pooled[...], wop[:, cols], preferred_element_type=f32)

    q_got("upf").wait_recv()
    q_got("dnf").wait_recv()
    q_sib(2).start()
    for i in (8, 9, 10, 13):
        loads[i].wait()
    for i in range(3):
        q_sib_got(i).wait_recv()
    q_pre = jnp.dot(hidden[...], wq[...], preferred_element_type=f32).astype(bf16)
    q_lat[...] = scaled_rows(q_pre.astype(f32), q_gain_s[...], QR).astype(bf16)
    q_nope[...] = jnp.dot(q_lat[...], wqn[...], preferred_element_type=f32).astype(bf16)
    q_rot = jnp.dot(q_lat[...], wqr[...], preferred_element_type=f32).astype(bf16).astype(f32)
    lane = lax.broadcasted_iota(jnp.int32, (TOK, 128), 1)
    for h in range(HEADS):
        rows = slice(h * TOK, (h + 1) * TOK)
        if h % 2 == 0:
            pair = turned(q_rot[:, h * 64 : h * 64 + 128], cos_s[...], sin_s[...]) * SCALE
        keep = lane < 64 if h % 2 == 0 else lane >= 64
        q_all[rows, KR:] = jnp.where(keep, pair, 0.0).astype(bf16)
        head = slice(h * NOPE_DIM, (h + 1) * NOPE_DIM)
        absorbed = lax.dot_general(
            q_nope[:, head], wku[:, head], (((1,), (1,)), ((), ())), preferred_element_type=f32
        )
        q_all[rows, :KR] = (absorbed * SCALE).astype(bf16)

    @pl.when(c == 0)
    def _():
        acquire_own(0, 1)
        acquire_own(0, 2)

    @pl.when(c == 1)
    def _():
        for i in (1, 7, 2, 6, 3, 5, 4):
            first1_got(i).wait_recv()
        for copy in sends_after(1, 0):
            copy.start()
        sib(1, 0).start()
        sib(1, 1).start()

    steps = 2 * (SEQ // 2) // STEP

    def row_of(i):
        cls = lax.rem(i + c, 2)
        return pl.multiple_of(cls * (SEQ // 2) + (i // 2) * STEP, STEP)

    def acquire(i):
        for m in range(1, 4):
            for cls in range(2):

                @pl.when((i == 2 * m) & (c == cls))
                def _():
                    for n in (2 * m, 2 * m + 1):
                        if n > 2 or cls == 1:
                            acquire_own(cls, n)

        @pl.when(lax.rem(i, 2) == 1)
        def _():
            for n in range(2):
                at = (1 - c) * (SEQ // 2) + (i // 2) * STEP + n * UNIT
                view = kv.at[pl.ds(at, UNIT)]
                remote(view, view, sib_ss.at[i - 1 + n], sib_rs.at[i - 1 + n], other).wait_recv()

    def scores(i, h):
        s_scr[h % 2] = lax.dot_general(
            q_all[h * MB : (h + 1) * MB, :],
            kv[pl.ds(row_of(i), STEP), :],
            (((1,), (1,)), ((), ())),
            preferred_element_type=f32,
        )

    def softmax(h):
        for r in range(0, MB, SUB):
            g = slice(h * MB + r, h * MB + r + SUB)
            s = [s_scr[h % 2, r : r + SUB, j * 128 : (j + 1) * 128] for j in range(STEP // 128)]
            m_old = m_s[g, :]
            top = s[0]
            for t in s[1:]:
                top = jnp.maximum(top, t)
            m_new = jnp.maximum(m_old, jnp.max(top, axis=1, keepdims=True))
            alpha = jnp.exp2(m_old - m_new)
            total = l_s[g, :] * alpha
            for j, t in enumerate(s):
                p = jnp.exp2(t - m_new)
                total = total + p
                p_scr[h % 2, r : r + SUB, j * 128 : (j + 1) * 128] = p.astype(bf16)
            m_s[g, :] = m_new
            l_s[g, :] = total
            for j in range(2):
                cols = slice(j * 128, (j + 1) * 128)
                acc[g, cols] = acc[g, cols] * alpha

    def product(i, h):
        g = slice(h * MB, (h + 1) * MB)
        acc[g, :] = acc[g, :] + jnp.dot(p_scr[h % 2], kv[pl.ds(row_of(i), STEP), :KR], preferred_element_type=f32)

    chunks = ROWS // MB
    zero = jnp.int32(0)
    scores(zero, 0)
    for h in range(chunks - 1):
        scores(zero, h + 1)
        softmax(h)
        if h > 0:
            product(zero, h - 1)

    def step(i, carry):
        acquire(i + 1)
        scores(i + 1, 0)
        softmax(chunks - 1)
        product(i, chunks - 2)
        for h in range(chunks - 1):
            scores(i + 1, h + 1)
            softmax(h)
            if h == 0:
                product(i, chunks - 1)
            else:
                product(i + 1, h - 1)
        return carry

    lax.fori_loop(0, steps - 1, step, 0)
    end = jnp.int32(steps - 1)
    softmax(chunks - 1)
    product(end, chunks - 2)
    product(end, chunks - 1)

    loads[11].wait()
    loads[12].wait()
    for h in range(HEADS):
        rows = slice(h * TOK, (h + 1) * TOK)
        head = slice(h * VALUE_DIM, (h + 1) * VALUE_DIM)
        total = jnp.sum(l_s[rows, :], axis=1, keepdims=True)
        weighted = (acc[rows, :] / total).astype(bf16)
        att[:, head] = jnp.dot(weighted, wvu[:, head], preferred_element_type=f32).astype(bf16)

    theirs = pl.ds((1 - c) * HALF, HALF)

    def share(j):
        return remote(send_buf.at[j], recv_buf.at[j], out_ss.at[j], out_rs.at[j], other)

    for j in range(4):
        cols = slice(j * 512, (j + 1) * 512)
        out_sum[:, cols] = out_sum[:, cols] + jnp.dot(att[...], woa[:, cols], preferred_element_type=f32)
        send_buf[j] = out_sum[theirs, cols].astype(bf16)
        share(j).start()
    for j in range(4):
        cols = slice(j * 512, (j + 1) * 512)
        share(j).wait_recv()
        out[:, cols] = (out_sum[mine, cols] + recv_buf[j].astype(f32)).astype(bf16)

    tok_copy.wait_send()
    gain_copy.wait_send()
    for name in ("up1", "up2", "dn1", "dn2", "upf", "dnf"):
        q_send(name).wait_send()
    for i in range(3):
        q_sib(i).wait_send()
    halo_next.wait_send()
    halo_prev.wait_send()
    for j in range(4):
        share(j).wait_send()

    @pl.when(c == 0)
    def _():
        for i in range(1, NX):
            first0(i).wait_send()
        for n in range(8):
            for copy in sends_after(0, n):
                copy.wait_send()
            sib(0, n).wait_send()

    @pl.when(c == 1)
    def _():
        for name in ("up1", "up2", "dn1", "dn2", "upf", "dnf"):
            kv_send(name).wait_send()
        for i in range(3):
            kv_sib(i).wait_send()
        for i in range(1, NZ):
            first1(i).wait_send()
        for n in range(8):
            for copy in sends_after(1, n):
                copy.wait_send()
            sib(1, n).wait_send()


def on_device(
    tokens,
    norm_gain,
    w_q_down,
    q_gain,
    w_q_nope,
    w_q_rope,
    w_kv_down,
    kv_gain,
    w_k_up,
    w_v_up,
    w_k_rope,
    w_pool_in,
    w_pool_mix,
    w_out_attn,
    w_out_pool,
):
    row_table, col_table = rope_tables()
    anywhere = pl.BlockSpec(memory_space=pl.ANY)
    vmem = pl.BlockSpec(memory_space=pltpu.VMEM)
    dma = pltpu.SemaphoreType.DMA
    result = pl.pallas_call(
        layer_body,
        out_shape=jax.ShapeDtypeStruct((HALF, D), bf16),
        in_specs=[anywhere] * 17,
        out_specs=vmem,
        scratch_shapes=[
            pltpu.VMEM((2, TOK, 1024), bf16),
            pltpu.VMEM((2, 8, 128), bf16),
            pltpu.VMEM((1, QR), f32),
            pltpu.VMEM((1, KR), f32),
            pltpu.VMEM((2, SEQ // GRID_W, 128), f32),
            pltpu.VMEM((2, GRID_W, 128), f32),
            pltpu.VMEM((TOK, D), bf16),
            pltpu.VMEM((D, KR), bf16),
            pltpu.VMEM((D, QR), bf16),
            pltpu.VMEM((ROPE_DIM, D), bf16),
            pltpu.VMEM((D, 512), bf16),
            pltpu.VMEM((QR, 1024), bf16),
            pltpu.VMEM((QR, 512), bf16),
            pltpu.VMEM((KR, 1024), bf16),
            pltpu.VMEM((KR, 1024), bf16),
            pltpu.VMEM((2, POOL_GROUP, POOL_GROUP), bf16),
            pltpu.VMEM((1024, D), bf16),
            pltpu.VMEM((512, D), bf16),
            pltpu.VMEM((TOK, 128), f32),
            pltpu.VMEM((TOK, 128), f32),
            pltpu.VMEM((SEQ, WIDE), bf16),
            pltpu.VMEM((ROWS, WIDE), bf16),
            pltpu.VMEM((TOK, QR), bf16),
            pltpu.VMEM((TOK, 1024), bf16),
            pltpu.VMEM((TOK, 512), bf16),
            pltpu.VMEM((32, 512), bf16),
            pltpu.VMEM((TOK, 512), bf16),
            pltpu.VMEM((TOK, D), f32),
            pltpu.VMEM((TOK, 1024), bf16),
            pltpu.VMEM((4, HALF, 512), bf16),
            pltpu.VMEM((4, HALF, 512), bf16),
            pltpu.VMEM((2, MB, STEP), f32),
            pltpu.VMEM((2, MB, STEP), bf16),
            pltpu.VMEM((ROWS, KR), f32),
            pltpu.VMEM((ROWS, 128), f32),
            pltpu.VMEM((ROWS, 128), f32),
            dma((17,)),
            dma((2,)),
            dma((2,)),
            dma((2, 6)),
            dma((2, 6)),
            dma((2, 3)),
            dma((2, 3)),
            dma((8,)),
            dma((8,)),
            dma((9,)),
            dma((9,)),
            dma((8,)),
            dma((8,)),
            dma((2,)),
            dma((2,)),
            dma((4,)),
            dma((4,)),
        ],
        compiler_params=pltpu.CompilerParams(
            collective_id=0, has_side_effects=True, vmem_limit_bytes=60 * 2**20
        ),
    )(
        tokens[0],
        norm_gain.reshape(8, 128),
        w_q_down,
        q_gain[None],
        w_q_nope,
        w_q_rope,
        w_kv_down,
        kv_gain[None],
        w_k_up,
        w_v_up,
        w_k_rope.T,
        w_pool_in,
        w_pool_mix,
        w_out_attn,
        w_out_pool,
        jnp.asarray(row_table),
        jnp.asarray(col_table),
    )
    return result[None]


def solution(mesh):
    torus = Mesh(
        mesh.devices.reshape(NZ, NX, mesh.shape["fs"], mesh.shape["tp"]), ("sp_0", "sp_1", "fs", "tp")
    )
    placed = (
        P("fs", SP, "tp"),
        P("tp"),
        P("fs", None),
        P(),
        P(None, "tp"),
        P(None, "tp"),
        P("fs", None),
        P(),
        P(None, "tp"),
        P(None, "tp"),
        P(),
        P(None, "tp"),
        P(),
        P("tp", None),
        P("tp", None),
    )
    return jax.shard_map(
        on_device, mesh=torus, in_specs=placed, out_specs=P("fs", SP_TP, None), check_vma=False
    )
```

```python
import functools

import jax
import jax.numpy as jnp
import numpy as np
from jax import lax
from jax.experimental import pallas as pl
from jax.experimental.pallas import tpu as pltpu
from jax.sharding import Mesh
from jax.sharding import PartitionSpec as P

NOPE_DIM = 128
ROPE_DIM = 64
VALUE_DIM = 128
GRID_W = 64
POOL_GROUP = 256
SP = ("sp_0", "sp_1")
SP_TP = ("sp_0", "sp_1", "tp")
EPS = 1e-06
THETA = 10000.0
LOG2E = 1.4426950408889634
MESH = pl.DeviceIdType.MESH

NZ, NX, NY = 8, 4, 4
TOK = 192
HALF = 96
D = 2048
HEADS = 8
QR, KR = 512, 256
WIDE = 384
UNIT = 384
ROWS = HEADS * TOK
MB = 384
STEP = 2 * UNIT
SUB = 32
SEQ = NZ * NX * TOK
SCALE = (NOPE_DIM + ROPE_DIM) ** (-0.5) * LOG2E
f32, bf16 = jnp.float32, jnp.bfloat16


def rope_tables():
    inverse = (THETA ** (-np.arange(0, ROPE_DIM // 2, 2) / (ROPE_DIM // 2))).astype(np.float32)
    lane = np.arange(128)
    freq = inverse[lane % 16]
    by_row = (lane // 32) % 2 == 0
    sign = np.where((lane // 16) % 2 == 0, -1.0, 1.0)

    def table(count, keep):
        angle = (np.arange(count, dtype=np.float32)[:, None] * freq).astype(np.float64)
        cos = np.where(keep, np.cos(angle), 0.0)
        sin = np.where(keep, np.sin(angle) * sign, 0.0)
        return np.stack([cos, sin]).astype(np.float32)

    return table(SEQ // GRID_W, by_row), table(GRID_W, ~by_row)


def turned(values, cos, sin):
    lane = lax.broadcasted_iota(jnp.int32, values.shape, 1)
    ahead = pltpu.roll(values, 112, 1)
    behind = pltpu.roll(values, 16, 1)
    partner = jnp.where((lane // 16) % 2 == 0, ahead, behind)
    return values * cos + partner * sin


def scaled_rows(values, gain, width):
    mean = jnp.sum(values * values, axis=1, keepdims=True) * (1.0 / width)
    return values * lax.rsqrt(mean + EPS) * gain


def layer_body(
    tokens,
    norm_gain,
    w_q_down,
    q_gain,
    w_q_nope,
    w_q_rope,
    w_kv_down,
    kv_gain,
    w_k_up,
    w_v_up,
    w_k_rope,
    w_pool_in,
    w_pool_mix,
    w_out_attn,
    w_out_pool,
    row_hbm,
    col_hbm,
    out,
    tok,
    gains,
    q_gain_s,
    kv_gain_s,
    row_table,
    col_table,
    hidden,
    wkv,
    wq,
    wkr,
    wpi,
    wqn,
    wqr,
    wku,
    wvu,
    mix,
    woa,
    wop,
    cos_s,
    sin_s,
    kv,
    q_all,
    q_lat,
    q_nope,
    pool_in,
    halo,
    pooled,
    out_sum,
    att,
    send_buf,
    recv_buf,
    s_scr,
    p_scr,
    acc,
    m_s,
    l_s,
    loc,
    tok_ss,
    tok_rs,
    w_ss,
    w_rs,
    ws_ss,
    ws_rs,
    p1_ss,
    p1_rs,
    ring_ss,
    ring_rs,
    sib_ss,
    sib_rs,
    halo_ss,
    halo_rs,
    out_ss,
    out_rs,
):
    z, x = lax.axis_index("sp_0"), lax.axis_index("sp_1")
    y, c = lax.axis_index("fs"), lax.axis_index("tp")
    sp = z * NX + x
    other = {"tp": 1 - c}
    y_up, y_down = {"fs": lax.rem(y + 1, NY)}, {"fs": lax.rem(y + NY - 1, NY)}
    z_up, z_down = {"sp_0": lax.rem(z + 1, NZ)}, {"sp_0": lax.rem(z + NZ - 1, NZ)}
    x_up, x_down = {"sp_1": lax.rem(x + 1, NX)}, {"sp_1": lax.rem(x + NX - 1, NX)}
    sp_next, sp_prev = lax.rem(sp + 1, NZ * NX), lax.rem(sp + NZ * NX - 1, NZ * NX)
    next_dev = {"sp_0": sp_next // NX, "sp_1": sp_next % NX}
    prev_dev = {"sp_0": sp_prev // NX, "sp_1": sp_prev % NX}

    def remote(src, dst, ssem, rsem, dev):
        return pltpu.make_async_remote_copy(
            src_ref=src, dst_ref=dst, send_sem=ssem, recv_sem=rsem, device_id=dev, device_id_type=MESH
        )

    barrier = pltpu.get_barrier_semaphore()
    partners = [other, y_up, y_down, next_dev, prev_dev]
    partners += [{"sp_0": lax.rem(z + i, NZ)} for i in range(1, NZ)]
    partners += [{"sp_1": lax.rem(x + i, NX)} for i in range(1, NX)]
    for dev in partners:
        pl.semaphore_signal(barrier, inc=1, device_id=dev, device_id_type=MESH)

    def local(i, src, dst):
        return pltpu.make_async_copy(src, dst, loc.at[i])

    loads = [
        local(0, tokens, tok.at[c]),
        local(1, norm_gain, gains.at[c]),
        local(2, w_kv_down, wkv.at[pl.ds(y * 512, 512)]),
        local(3, w_k_rope, wkr),
        local(4, w_pool_in, wpi),
        local(5, w_q_down, wq.at[pl.ds(y * 512, 512)]),
        local(6, w_pool_mix.at[pl.ds(2 * c, 2)], mix),
        local(7, w_out_pool, wop),
        local(8, w_q_nope, wqn),
        local(9, w_q_rope, wqr),
        local(10, w_k_up, wku),
        local(11, w_v_up, wvu),
        local(12, w_out_attn, woa),
        local(13, q_gain, q_gain_s),
        local(14, kv_gain, kv_gain_s),
        local(15, row_hbm, row_table),
        local(16, col_hbm, col_table),
    ]
    for i in (0, 1, 2, 15, 16, 5):
        loads[i].start()

    m_s[...] = jnp.full(m_s.shape, -1e30, f32)
    l_s[...] = jnp.zeros(l_s.shape, f32)
    acc[...] = jnp.zeros(acc.shape, f32)
    pl.semaphore_wait(barrier, len(partners))

    tok_copy = remote(tok.at[c], tok.at[c], tok_ss.at[0], tok_rs.at[0], other)
    gain_copy = remote(gains.at[c], gains.at[c], tok_ss.at[1], tok_rs.at[1], other)
    loads[0].wait()
    loads[1].wait()
    tok_copy.start()
    gain_copy.start()

    y1, y2, y3 = lax.rem(y + 3, NY), lax.rem(y + 1, NY), lax.rem(y + 2, NY)

    def weight_copies(w, buf, base, part):
        def rows(of, p):
            return buf.at[pl.ds(of * 512 + base + p * part, part)]

        ss, rs = w_ss.at[w], w_rs.at[w]

        def copy(i, of, p, dev):
            return remote(rows(of, p), rows(of, p), ss.at[i], rs.at[i], dev)

        def sends(name):
            return {
                "up1": lambda: copy(0, y, 0, y_up),
                "up2": lambda: copy(1, y, 1, y_up),
                "dn1": lambda: copy(2, y, 1, y_down),
                "dn2": lambda: copy(3, y, 0, y_down),
                "upf": lambda: copy(4, y1, 0, y_up),
                "dnf": lambda: copy(5, y2, 1, y_down),
            }[name]()

        def got(name):
            return {
                "up1": lambda: copy(0, y1, 0, y_up),
                "up2": lambda: copy(1, y1, 1, y_up),
                "dn1": lambda: copy(2, y2, 1, y_up),
                "dn2": lambda: copy(3, y2, 0, y_up),
                "upf": lambda: copy(4, y3, 0, y_up),
                "dnf": lambda: copy(5, y3, 1, y_up),
            }[name]()

        return sends, got

    def weight_sibling(w, buf, base, count, i):
        view = buf.at[pl.ds((y1, y2, y3)[i] * 512 + base, count)]
        return remote(view, view, ws_ss.at[w, i], ws_rs.at[w, i], other)

    kv_send, kv_got = weight_copies(0, wkv, 0, 256)
    q_send, q_got = weight_copies(1, wq, c * 256, 128)

    def kv_sib(i):
        return weight_sibling(0, wkv, 0, 512, i)

    def q_sib(i):
        return weight_sibling(1, wq, c * 256, 256, i)

    def q_sib_got(i):
        return weight_sibling(1, wq, (1 - c) * 256, 256, i)

    def start_queries():
        for name in ("up1", "dn1", "up2", "dn2"):
            q_send(name).start()

    loads[2].wait()

    @pl.when(c == 1)
    def _():
        for name in ("up1", "dn1", "up2", "dn2"):
            kv_send(name).start()

    for i in (3, 4, 6, 7, 8, 9, 10, 11, 13, 14, 12):
        loads[i].start()
    loads[5].wait()

    loads[15].wait()
    loads[16].wait()
    for k in range(TOK // GRID_W):
        rows = slice(k * GRID_W, (k + 1) * GRID_W)
        at = 3 * sp + k
        cos_s[rows, :] = row_table[0, pl.ds(at, 1), :] + col_table[0]
        sin_s[rows, :] = row_table[1, pl.ds(at, 1), :] + col_table[1]

    remote(tok.at[1 - c], tok.at[1 - c], tok_ss.at[0], tok_rs.at[0], other).wait_recv()
    remote(gains.at[1 - c], gains.at[1 - c], tok_ss.at[1], tok_rs.at[1], other).wait_recv()
    gain = [gains[half].astype(f32) for half in range(2)]
    for r in range(0, TOK, 16):
        parts = [tok[half, r : r + 16, :].astype(f32) for half in range(2)]
        total = jnp.sum(parts[0] * parts[0] + parts[1] * parts[1], axis=1, keepdims=True)
        inv = lax.rsqrt(total * (1.0 / D) + EPS)
        for half in range(2):
            for j in range(8):
                cols = slice(j * 128, (j + 1) * 128)
                at = half * 1024 + j * 128
                hidden[r : r + 16, at : at + 128] = (parts[half][:, cols] * inv * gain[half][j : j + 1, :]).astype(bf16)
    @pl.when(c == 1)
    def _():
        kv_got("up1").wait_recv()
        kv_send("upf").start()
        kv_got("dn1").wait_recv()
        kv_send("dnf").start()
        start_queries()
        kv_got("up2").wait_recv()
        kv_sib(0).start()
        kv_got("dn2").wait_recv()
        kv_sib(1).start()

    @pl.when(c == 0)
    def _():
        kv_sib(0).wait_recv()
        start_queries()
        kv_sib(1).wait_recv()

    loads[4].wait()
    pool_in[...] = jnp.dot(hidden[...], wpi[...], preferred_element_type=f32).astype(bf16)
    halo_next = remote(pool_in.at[pl.ds(TOK - 16, 16)], halo.at[pl.ds(0, 16)], halo_ss.at[0], halo_rs.at[0], next_dev)
    halo_prev = remote(pool_in.at[pl.ds(0, 16)], halo.at[pl.ds(16, 16)], halo_ss.at[1], halo_rs.at[1], prev_dev)
    halo_next.start()
    halo_prev.start()

    mine = pl.ds(c * HALF, HALF)
    loads[3].wait()
    key_pre = lax.dot_general(
        hidden[mine, :], wkr[...], (((1,), (1,)), ((), ())), preferred_element_type=f32
    )
    key_pre = jnp.concatenate([key_pre, key_pre], axis=1).astype(bf16).astype(f32)
    key_rope = turned(key_pre, cos_s[mine, :], sin_s[mine, :]).astype(bf16)

    @pl.when(c == 1)
    def _():
        kv_got("upf").wait_recv()
        kv_got("dnf").wait_recv()
        kv_sib(2).start()

    @pl.when(c == 0)
    def _():
        kv_sib(2).wait_recv()

    loads[14].wait()
    kv_pre = jnp.dot(hidden[mine, :], wkv[...], preferred_element_type=f32).astype(bf16)
    own0 = x * HALF
    own1 = SEQ // 2 + z * HALF
    own_rows = pl.ds(pl.multiple_of(jnp.where(c == 1, own0, own1), HALF), HALF)
    kv[own_rows, :KR] = scaled_rows(kv_pre.astype(f32), kv_gain_s[...], KR).astype(bf16)
    kv[own_rows, KR:] = key_rope

    def blk0(xx):
        return kv.at[pl.ds(xx * HALF, HALF)]

    def blk1(zz):
        return kv.at[pl.ds(SEQ // 2 + zz * HALF, HALF)]

    def first0(i):
        to = lax.rem(x + i, NX)
        return remote(blk0(x), blk0(x), p1_ss.at[i], p1_rs.at[i], {"sp_1": to})

    def first0_got(i):
        view = blk0(lax.rem(x + NX - i, NX))
        return remote(view, view, p1_ss.at[i], p1_rs.at[i], x_up)

    def first1(i):
        to = lax.rem(z + i, NZ)
        return remote(blk1(z), blk1(z), p1_ss.at[i], p1_rs.at[i], {"sp_0": to})

    def first1_got(i):
        view = blk1(lax.rem(z + NZ - i, NZ))
        return remote(view, view, p1_ss.at[i], p1_rs.at[i], z_up)

    @pl.when(c == 1)
    def _():
        for i in (1, 3, 2):
            first0(i).start()

    @pl.when(c == 0)
    def _():
        for i in (1, 7, 2, 6, 3, 5, 4):
            first1(i).start()

    q_got("up1").wait_recv()
    q_send("upf").start()
    q_got("dn1").wait_recv()
    q_send("dnf").start()

    def unit(cls, n):
        return kv.at[pl.ds(cls * (SEQ // 2) + n * UNIT, UNIT)]

    def half_unit(n, h):
        return kv.at[pl.ds(n * UNIT + h * (UNIT // 2), UNIT // 2)]

    def ring(src, dst, i, dev):
        return remote(src, dst, ring_ss.at[i], ring_rs.at[i], dev)

    def sends_after(cls, n):
        if cls == 0:
            up, down = z_up, z_down
            if n == 0:
                return [ring(unit(0, 0), unit(0, 1), 1, up), ring(unit(0, 0), unit(0, 2), 2, down)]
            if n < 5:
                return [ring(unit(0, n), unit(0, n + 2), n + 2, up if n % 2 else down)]
            if n < 7:
                return [ring(half_unit(n, n - 5), half_unit(7, n - 5), n + 2, up if n % 2 else down)]
            return []
        up, down = x_up, x_down
        if n == 0:
            return [
                ring(unit(1, 0), unit(1, 2), 2, up),
                ring(unit(1, 1), unit(1, 3), 3, down),
                ring(unit(1, 1), unit(1, 4), 4, up),
                ring(unit(1, 0), unit(1, 5), 5, down),
            ]
        if n == 2:
            return [ring(unit(1, 2), unit(1, 6), 6, up)]
        if n == 3:
            return [ring(unit(1, 3), unit(1, 7), 7, down)]
        return []

    def arrivals_for(cls, n):
        if cls == 0 and n == 7:
            return [ring(half_unit(7, h), half_unit(7, h), 7 + h, z_up) for h in range(2)]
        return [ring(unit(cls, n), unit(cls, n), n, z_up)]

    def sib(cls, n):
        return remote(unit(cls, n), unit(cls, n), sib_ss.at[n], sib_rs.at[n], other)

    def acquire_own(cls, n):
        for copy in arrivals_for(cls, n):
            copy.wait_recv()
        for copy in sends_after(cls, n):
            copy.start()
        sib(cls, n).start()

    @pl.when(c == 1)
    def _():
        for i in (1, 3, 2):
            first0_got(i).wait_recv()
        for copy in sends_after(0, 0):
            copy.start()
        sib(0, 0).start()


    q_got("up2").wait_recv()
    q_sib(0).start()
    q_got("dn2").wait_recv()
    q_sib(1).start()

    remote(halo.at[pl.ds(0, 16)], halo.at[pl.ds(0, 16)], halo_ss.at[0], halo_rs.at[0], next_dev).wait_recv()
    remote(halo.at[pl.ds(16, 16)], halo.at[pl.ds(16, 16)], halo_ss.at[1], halo_rs.at[1], next_dev).wait_recv()
    loads[6].wait()
    loads[7].wait()
    row_i = lax.broadcasted_iota(jnp.int32, (TOK, TOK), 0)
    gap = lax.broadcasted_iota(jnp.int32, (TOK, TOK), 1) - row_i
    rim_row = lax.broadcasted_iota(jnp.int32, (TOK, 32), 0)
    rim_col = lax.broadcasted_iota(jnp.int32, (TOK, 32), 1)
    before = rim_col < 16
    rim_gap = jnp.where(before, rim_col - 16, rim_col - 16 + TOK) - rim_row
    rim_ok = (before & (sp > 0)) | (~before & (sp < NZ * NX - 1))
    place = lax.broadcasted_iota(jnp.int32, (TOK, POOL_GROUP), 0) + sp * TOK
    for g in range(2):
        span = (1 + 3 * c) * (1 + g)
        cols = slice(g * POOL_GROUP, (g + 1) * POOL_GROUP)
        near = ((gap >= -span) & (gap < span)).astype(f32).astype(bf16)
        rim = ((rim_gap >= -span) & (rim_gap < span) & rim_ok).astype(f32).astype(bf16)
        sums = jnp.dot(near, pool_in[:, cols], preferred_element_type=f32)
        sums = sums + jnp.dot(rim, halo[:, cols], preferred_element_type=f32)
        low = jnp.maximum(place - span, 0)
        high = jnp.minimum(place + span, SEQ)
        mean = (sums / (high - low).astype(f32)).astype(bf16)
        spread = (mean.astype(f32) - pool_in[:, cols].astype(f32)).astype(bf16)
        pooled[:, cols] = jnp.dot(spread, mix[g], preferred_element_type=f32).astype(bf16)
    for j in range(4):
        cols = slice(j * 512, (j + 1) * 512)
        out_sum[:, cols] = jnp.dot(pooled[...], wop[:, cols], preferred_element_type=f32)

    q_got("upf").wait_recv()
    q_got("dnf").wait_recv()
    q_sib(2).start()
    for i in (8, 9, 10, 13):
        loads[i].wait()
    @pl.when(c == 0)
    def _():
        for i in (1, 7, 2, 6, 3, 5, 4):
            first1_got(i).wait_recv()
        for copy in sends_after(1, 0):
            copy.start()
        sib(1, 0).start()
        sib(1, 1).start()

    for i in range(3):
        q_sib_got(i).wait_recv()
    q_pre = jnp.dot(hidden[...], wq[...], preferred_element_type=f32).astype(bf16)
    q_lat[...] = scaled_rows(q_pre.astype(f32), q_gain_s[...], QR).astype(bf16)
    q_nope[...] = jnp.dot(q_lat[...], wqn[...], preferred_element_type=f32).astype(bf16)
    q_rot = jnp.dot(q_lat[...], wqr[...], preferred_element_type=f32).astype(bf16).astype(f32)
    lane = lax.broadcasted_iota(jnp.int32, (TOK, 128), 1)
    for h in range(HEADS):
        rows = slice(h * TOK, (h + 1) * TOK)
        if h % 2 == 0:
            pair = turned(q_rot[:, h * 64 : h * 64 + 128], cos_s[...], sin_s[...]) * SCALE
        keep = lane < 64 if h % 2 == 0 else lane >= 64
        q_all[rows, KR:] = jnp.where(keep, pair, 0.0).astype(bf16)
        head = slice(h * NOPE_DIM, (h + 1) * NOPE_DIM)
        absorbed = lax.dot_general(
            q_nope[:, head], wku[:, head], (((1,), (1,)), ((), ())), preferred_element_type=f32
        )
        q_all[rows, :KR] = (absorbed * SCALE).astype(bf16)

    @pl.when(c == 1)
    def _():
        acquire_own(0, 1)
        acquire_own(0, 2)

    steps = 2 * (SEQ // 2) // STEP

    def row_of(i):
        cls = lax.rem(i + 1 - c, 2)
        return pl.multiple_of(cls * (SEQ // 2) + (i // 2) * STEP, STEP)

    def acquire(i):
        for m in range(1, 4):

            @pl.when((i == 2 * m) & (c == 1))
            def _():
                for n in (2 * m + 1, 2 * m + 2):
                    if n < 8:
                        acquire_own(0, n)

            @pl.when((i == 2 * m) & (c == 0))
            def _():
                for n in (2 * m, 2 * m + 1):
                    acquire_own(1, n)

        @pl.when(lax.rem(i, 2) == 1)
        def _():
            for n in range(2):
                at = c * (SEQ // 2) + (i // 2) * STEP + n * UNIT
                view = kv.at[pl.ds(at, UNIT)]
                remote(view, view, sib_ss.at[i - 1 + n], sib_rs.at[i - 1 + n], other).wait_recv()

    def scores(i, h):
        s_scr[h % 2] = lax.dot_general(
            q_all[h * MB : (h + 1) * MB, :],
            kv[pl.ds(row_of(i), STEP), :],
            (((1,), (1,)), ((), ())),
            preferred_element_type=f32,
        )

    def softmax(h):
        for r in range(0, MB, SUB):
            g = slice(h * MB + r, h * MB + r + SUB)
            s = [s_scr[h % 2, r : r + SUB, j * 128 : (j + 1) * 128] for j in range(STEP // 128)]
            m_old = m_s[g, :]
            top = s[0]
            for t in s[1:]:
                top = jnp.maximum(top, t)
            m_new = jnp.maximum(m_old, jnp.max(top, axis=1, keepdims=True))
            alpha = jnp.exp2(m_old - m_new)
            total = l_s[g, :] * alpha
            for j, t in enumerate(s):
                p = jnp.exp2(t - m_new)
                total = total + p
                p_scr[h % 2, r : r + SUB, j * 128 : (j + 1) * 128] = p.astype(bf16)
            m_s[g, :] = m_new
            l_s[g, :] = total
            for j in range(2):
                cols = slice(j * 128, (j + 1) * 128)
                acc[g, cols] = acc[g, cols] * alpha

    def product(i, h):
        g = slice(h * MB, (h + 1) * MB)
        acc[g, :] = acc[g, :] + jnp.dot(p_scr[h % 2], kv[pl.ds(row_of(i), STEP), :KR], preferred_element_type=f32)

    chunks = ROWS // MB
    zero = jnp.int32(0)
    scores(zero, 0)
    for h in range(chunks - 1):
        scores(zero, h + 1)
        softmax(h)
        if h > 0:
            product(zero, h - 1)

    def step(i, carry):
        acquire(i + 1)
        scores(i + 1, 0)
        softmax(chunks - 1)
        product(i, chunks - 2)
        for h in range(chunks - 1):
            scores(i + 1, h + 1)
            softmax(h)
            if h == 0:
                product(i, chunks - 1)
            else:
                product(i + 1, h - 1)
        return carry

    lax.fori_loop(0, steps - 1, step, 0)
    end = jnp.int32(steps - 1)
    softmax(chunks - 1)
    product(end, chunks - 2)
    product(end, chunks - 1)

    loads[11].wait()
    loads[12].wait()
    for h in range(HEADS):
        rows = slice(h * TOK, (h + 1) * TOK)
        head = slice(h * VALUE_DIM, (h + 1) * VALUE_DIM)
        total = jnp.sum(l_s[rows, :], axis=1, keepdims=True)
        weighted = (acc[rows, :] / total).astype(bf16)
        att[:, head] = jnp.dot(weighted, wvu[:, head], preferred_element_type=f32).astype(bf16)

    theirs = pl.ds((1 - c) * HALF, HALF)

    def share(j):
        return remote(send_buf.at[j], recv_buf.at[j], out_ss.at[j], out_rs.at[j], other)

    def projected(rows, cols):
        return out_sum[rows, cols] + jnp.dot(att[rows, :], woa[:, cols], preferred_element_type=f32)

    blocks = [slice(j * 512, (j + 1) * 512) for j in range(4)]
    for j, cols in enumerate(blocks):
        send_buf[j] = projected(theirs, cols).astype(bf16)
        share(j).start()
    for cols in blocks:
        out_sum[mine, cols] = projected(mine, cols)
    for j, cols in enumerate(blocks):
        share(j).wait_recv()
        out[:, cols] = (out_sum[mine, cols] + recv_buf[j].astype(f32)).astype(bf16)

    tok_copy.wait_send()
    gain_copy.wait_send()
    for name in ("up1", "up2", "dn1", "dn2", "upf", "dnf"):
        q_send(name).wait_send()
    for i in range(3):
        q_sib(i).wait_send()
    halo_next.wait_send()
    halo_prev.wait_send()
    for j in range(4):
        share(j).wait_send()

    @pl.when(c == 1)
    def _():
        for name in ("up1", "up2", "dn1", "dn2", "upf", "dnf"):
            kv_send(name).wait_send()
        for i in range(3):
            kv_sib(i).wait_send()
        for i in range(1, NX):
            first0(i).wait_send()
        for n in range(8):
            for copy in sends_after(0, n):
                copy.wait_send()
            sib(0, n).wait_send()

    @pl.when(c == 0)
    def _():
        for i in range(1, NZ):
            first1(i).wait_send()
        for n in range(8):
            for copy in sends_after(1, n):
                copy.wait_send()
            sib(1, n).wait_send()


def on_device(
    tokens,
    norm_gain,
    w_q_down,
    q_gain,
    w_q_nope,
    w_q_rope,
    w_kv_down,
    kv_gain,
    w_k_up,
    w_v_up,
    w_k_rope,
    w_pool_in,
    w_pool_mix,
    w_out_attn,
    w_out_pool,
):
    row_table, col_table = rope_tables()
    anywhere = pl.BlockSpec(memory_space=pl.ANY)
    vmem = pl.BlockSpec(memory_space=pltpu.VMEM)
    dma = pltpu.SemaphoreType.DMA
    result = pl.pallas_call(
        layer_body,
        out_shape=jax.ShapeDtypeStruct((HALF, D), bf16),
        in_specs=[anywhere] * 17,
        out_specs=vmem,
        scratch_shapes=[
            pltpu.VMEM((2, TOK, 1024), bf16),
            pltpu.VMEM((2, 8, 128), bf16),
            pltpu.VMEM((1, QR), f32),
            pltpu.VMEM((1, KR), f32),
            pltpu.VMEM((2, SEQ // GRID_W, 128), f32),
            pltpu.VMEM((2, GRID_W, 128), f32),
            pltpu.VMEM((TOK, D), bf16),
            pltpu.VMEM((D, KR), bf16),
            pltpu.VMEM((D, QR), bf16),
            pltpu.VMEM((ROPE_DIM, D), bf16),
            pltpu.VMEM((D, 512), bf16),
            pltpu.VMEM((QR, 1024), bf16),
            pltpu.VMEM((QR, 512), bf16),
            pltpu.VMEM((KR, 1024), bf16),
            pltpu.VMEM((KR, 1024), bf16),
            pltpu.VMEM((2, POOL_GROUP, POOL_GROUP), bf16),
            pltpu.VMEM((1024, D), bf16),
            pltpu.VMEM((512, D), bf16),
            pltpu.VMEM((TOK, 128), f32),
            pltpu.VMEM((TOK, 128), f32),
            pltpu.VMEM((SEQ, WIDE), bf16),
            pltpu.VMEM((ROWS, WIDE), bf16),
            pltpu.VMEM((TOK, QR), bf16),
            pltpu.VMEM((TOK, 1024), bf16),
            pltpu.VMEM((TOK, 512), bf16),
            pltpu.VMEM((32, 512), bf16),
            pltpu.VMEM((TOK, 512), bf16),
            pltpu.VMEM((TOK, D), f32),
            pltpu.VMEM((TOK, 1024), bf16),
            pltpu.VMEM((4, HALF, 512), bf16),
            pltpu.VMEM((4, HALF, 512), bf16),
            pltpu.VMEM((2, MB, STEP), f32),
            pltpu.VMEM((2, MB, STEP), bf16),
            pltpu.VMEM((ROWS, KR), f32),
            pltpu.VMEM((ROWS, 128), f32),
            pltpu.VMEM((ROWS, 128), f32),
            dma((17,)),
            dma((2,)),
            dma((2,)),
            dma((2, 6)),
            dma((2, 6)),
            dma((2, 3)),
            dma((2, 3)),
            dma((8,)),
            dma((8,)),
            dma((9,)),
            dma((9,)),
            dma((8,)),
            dma((8,)),
            dma((2,)),
            dma((2,)),
            dma((4,)),
            dma((4,)),
        ],
        compiler_params=pltpu.CompilerParams(
            collective_id=0, has_side_effects=True, vmem_limit_bytes=60 * 2**20
        ),
    )(
        tokens[0],
        norm_gain.reshape(8, 128),
        w_q_down,
        q_gain[None],
        w_q_nope,
        w_q_rope,
        w_kv_down,
        kv_gain[None],
        w_k_up,
        w_v_up,
        w_k_rope.T,
        w_pool_in,
        w_pool_mix,
        w_out_attn,
        w_out_pool,
        jnp.asarray(row_table),
        jnp.asarray(col_table),
    )
    return result[None]


def solution(mesh):
    torus = Mesh(
        mesh.devices.reshape(NZ, NX, mesh.shape["fs"], mesh.shape["tp"]), ("sp_0", "sp_1", "fs", "tp")
    )
    placed = (
        P("fs", SP, "tp"),
        P("tp"),
        P("fs", None),
        P(),
        P(None, "tp"),
        P(None, "tp"),
        P("fs", None),
        P(),
        P(None, "tp"),
        P(None, "tp"),
        P(),
        P(None, "tp"),
        P(),
        P("tp", None),
        P("tp", None),
    )
    return jax.shard_map(
        on_device, mesh=torus, in_specs=placed, out_specs=P("fs", SP_TP, None), check_vma=False
    )
```

```python
import functools

import jax
import jax.numpy as jnp
import numpy as np
from jax import lax
from jax.experimental import pallas as pl
from jax.experimental.pallas import tpu as pltpu
from jax.sharding import Mesh
from jax.sharding import PartitionSpec as P

NOPE_DIM = 128
ROPE_DIM = 64
VALUE_DIM = 128
GRID_W = 64
POOL_GROUP = 256
SP = ("sp_0", "sp_1")
SP_TP = ("sp_0", "sp_1", "tp")
EPS = 1e-06
THETA = 10000.0
LOG2E = 1.4426950408889634
MESH = pl.DeviceIdType.MESH

NZ, NX, NY = 8, 4, 4
TOK = 192
HALF = 96
D = 2048
HEADS = 8
QR, KR = 512, 256
WIDE = 384
UNIT = 384
ROWS = HEADS * TOK
MB = 256
STEP = 2 * UNIT
SUB = 32
SEQ = NZ * NX * TOK
SCALE = (NOPE_DIM + ROPE_DIM) ** (-0.5) * LOG2E
f32, bf16 = jnp.float32, jnp.bfloat16


def rope_tables():
    inverse = (THETA ** (-np.arange(0, ROPE_DIM // 2, 2) / (ROPE_DIM // 2))).astype(np.float32)
    lane = np.arange(128)
    freq = inverse[lane % 16]
    by_row = (lane // 32) % 2 == 0
    sign = np.where((lane // 16) % 2 == 0, -1.0, 1.0)

    def table(count, keep):
        angle = (np.arange(count, dtype=np.float32)[:, None] * freq).astype(np.float64)
        cos = np.where(keep, np.cos(angle), 0.0)
        sin = np.where(keep, np.sin(angle) * sign, 0.0)
        return np.stack([cos, sin]).astype(np.float32)

    return table(SEQ // GRID_W, by_row), table(GRID_W, ~by_row)


def turned(values, cos, sin):
    lane = lax.broadcasted_iota(jnp.int32, values.shape, 1)
    ahead = pltpu.roll(values, 112, 1)
    behind = pltpu.roll(values, 16, 1)
    partner = jnp.where((lane // 16) % 2 == 0, ahead, behind)
    return values * cos + partner * sin


def scaled_rows(values, gain, width):
    mean = jnp.sum(values * values, axis=1, keepdims=True) * (1.0 / width)
    return values * lax.rsqrt(mean + EPS) * gain


def layer_body(
    tokens,
    norm_gain,
    w_q_down,
    q_gain,
    w_q_nope,
    w_q_rope,
    w_kv_down,
    kv_gain,
    w_k_up,
    w_v_up,
    w_k_rope,
    w_pool_in,
    w_pool_mix,
    w_out_attn,
    w_out_pool,
    row_hbm,
    col_hbm,
    out,
    tok,
    gains,
    q_gain_s,
    kv_gain_s,
    row_table,
    col_table,
    hidden,
    wkv,
    wq,
    wkr,
    wpi,
    wqn,
    wqr,
    wku,
    wvu,
    mix,
    woa,
    wop,
    cos_s,
    sin_s,
    kv,
    q_all,
    q_sum,
    q_lat,
    q_nope,
    pool_in,
    halo,
    pooled,
    out_sum,
    att,
    send_buf,
    recv_buf,
    s_scr,
    p_scr,
    acc,
    m_s,
    l_s,
    loc,
    tok_ss,
    tok_rs,
    w_ss,
    w_rs,
    ws_ss,
    ws_rs,
    p1_ss,
    p1_rs,
    ring_ss,
    ring_rs,
    sib_ss,
    sib_rs,
    halo_ss,
    halo_rs,
    out_ss,
    out_rs,
):
    z, x = lax.axis_index("sp_0"), lax.axis_index("sp_1")
    y, c = lax.axis_index("fs"), lax.axis_index("tp")
    sp = z * NX + x
    other = {"tp": 1 - c}
    y_up, y_down = {"fs": lax.rem(y + 1, NY)}, {"fs": lax.rem(y + NY - 1, NY)}
    z_up, z_down = {"sp_0": lax.rem(z + 1, NZ)}, {"sp_0": lax.rem(z + NZ - 1, NZ)}
    x_up, x_down = {"sp_1": lax.rem(x + 1, NX)}, {"sp_1": lax.rem(x + NX - 1, NX)}
    sp_next, sp_prev = lax.rem(sp + 1, NZ * NX), lax.rem(sp + NZ * NX - 1, NZ * NX)
    next_dev = {"sp_0": sp_next // NX, "sp_1": sp_next % NX}
    prev_dev = {"sp_0": sp_prev // NX, "sp_1": sp_prev % NX}

    def remote(src, dst, ssem, rsem, dev):
        return pltpu.make_async_remote_copy(
            src_ref=src, dst_ref=dst, send_sem=ssem, recv_sem=rsem, device_id=dev, device_id_type=MESH
        )

    barrier = pltpu.get_barrier_semaphore()
    partners = [other, y_up, y_down, next_dev, prev_dev]
    partners += [{"sp_0": lax.rem(z + i, NZ)} for i in range(1, NZ)]
    partners += [{"sp_1": lax.rem(x + i, NX)} for i in range(1, NX)]
    for dev in partners:
        pl.semaphore_signal(barrier, inc=1, device_id=dev, device_id_type=MESH)

    def local(i, src, dst):
        return pltpu.make_async_copy(src, dst, loc.at[i])

    loads = [
        local(0, tokens, tok.at[c]),
        local(1, norm_gain, gains.at[c]),
        local(2, w_kv_down, wkv.at[pl.ds(y * 512, 512)]),
        local(3, w_k_rope, wkr),
        local(4, w_pool_in, wpi),
        local(5, w_q_down, wq.at[pl.ds(y * 512, 512)]),
        local(6, w_pool_mix.at[pl.ds(2 * c, 2)], mix),
        local(7, w_out_pool, wop),
        local(8, w_q_nope, wqn),
        local(9, w_q_rope, wqr),
        local(10, w_k_up, wku),
        local(11, w_v_up, wvu),
        local(12, w_out_attn, woa),
        local(13, q_gain, q_gain_s),
        local(14, kv_gain, kv_gain_s),
        local(15, row_hbm, row_table),
        local(16, col_hbm, col_table),
    ]
    for i in (0, 1, 2, 15, 16, 5):
        loads[i].start()

    m_s[...] = jnp.full(m_s.shape, -1e30, f32)
    l_s[...] = jnp.zeros(l_s.shape, f32)
    acc[...] = jnp.zeros(acc.shape, f32)
    pl.semaphore_wait(barrier, len(partners))

    tok_copy = remote(tok.at[c], tok.at[c], tok_ss.at[0], tok_rs.at[0], other)
    gain_copy = remote(gains.at[c], gains.at[c], tok_ss.at[1], tok_rs.at[1], other)
    loads[0].wait()
    loads[1].wait()
    tok_copy.start()
    gain_copy.start()

    y1, y2, y3 = lax.rem(y + 3, NY), lax.rem(y + 1, NY), lax.rem(y + 2, NY)

    def weight_copies(w, buf, base, part):
        def rows(of, p):
            return buf.at[pl.ds(of * 512 + base + p * part, part)]

        ss, rs = w_ss.at[w], w_rs.at[w]

        def copy(i, of, p, dev):
            return remote(rows(of, p), rows(of, p), ss.at[i], rs.at[i], dev)

        def sends(name):
            return {
                "up1": lambda: copy(0, y, 0, y_up),
                "up2": lambda: copy(1, y, 1, y_up),
                "dn1": lambda: copy(2, y, 1, y_down),
                "dn2": lambda: copy(3, y, 0, y_down),
                "upf": lambda: copy(4, y1, 0, y_up),
                "dnf": lambda: copy(5, y2, 1, y_down),
            }[name]()

        def got(name):
            return {
                "up1": lambda: copy(0, y1, 0, y_up),
                "up2": lambda: copy(1, y1, 1, y_up),
                "dn1": lambda: copy(2, y2, 1, y_up),
                "dn2": lambda: copy(3, y2, 0, y_up),
                "upf": lambda: copy(4, y3, 0, y_up),
                "dnf": lambda: copy(5, y3, 1, y_up),
            }[name]()

        return sends, got

    def weight_sibling(w, buf, base, count, i):
        view = buf.at[pl.ds((y1, y2, y3)[i] * 512 + base, count)]
        return remote(view, view, ws_ss.at[w, i], ws_rs.at[w, i], other)

    kv_send, kv_got = weight_copies(0, wkv, 0, 256)
    q_send, q_got = weight_copies(1, wq, c * 256, 128)

    def kv_sib(i):
        return weight_sibling(0, wkv, 0, 512, i)

    def q_sib(i):
        return weight_sibling(1, wq, c * 256, 256, i)

    def q_sib_got(i):
        return weight_sibling(1, wq, (1 - c) * 256, 256, i)

    def start_queries():
        for name in ("up1", "dn1", "up2", "dn2"):
            q_send(name).start()

    loads[2].wait()

    @pl.when(c == 1)
    def _():
        for name in ("up1", "dn1", "up2", "dn2"):
            kv_send(name).start()

    for i in (3, 4, 6, 7, 8, 9, 10, 11, 13, 14, 12):
        loads[i].start()
    loads[5].wait()

    loads[15].wait()
    loads[16].wait()
    for k in range(TOK // GRID_W):
        rows = slice(k * GRID_W, (k + 1) * GRID_W)
        at = 3 * sp + k
        cos_s[rows, :] = row_table[0, pl.ds(at, 1), :] + col_table[0]
        sin_s[rows, :] = row_table[1, pl.ds(at, 1), :] + col_table[1]

    remote(tok.at[1 - c], tok.at[1 - c], tok_ss.at[0], tok_rs.at[0], other).wait_recv()
    remote(gains.at[1 - c], gains.at[1 - c], tok_ss.at[1], tok_rs.at[1], other).wait_recv()
    gain = [gains[half].astype(f32) for half in range(2)]
    for r in range(0, TOK, 16):
        parts = [tok[half, r : r + 16, :].astype(f32) for half in range(2)]
        total = jnp.sum(parts[0] * parts[0] + parts[1] * parts[1], axis=1, keepdims=True)
        inv = lax.rsqrt(total * (1.0 / D) + EPS)
        for half in range(2):
            for j in range(8):
                cols = slice(j * 128, (j + 1) * 128)
                at = half * 1024 + j * 128
                hidden[r : r + 16, at : at + 128] = (parts[half][:, cols] * inv * gain[half][j : j + 1, :]).astype(bf16)
    @pl.when(c == 1)
    def _():
        kv_got("up1").wait_recv()
        kv_send("upf").start()
        kv_got("dn1").wait_recv()
        kv_send("dnf").start()
        start_queries()
        kv_got("up2").wait_recv()
        kv_sib(0).start()
        kv_got("dn2").wait_recv()
        kv_sib(1).start()

    @pl.when(c == 0)
    def _():
        kv_sib(0).wait_recv()
        start_queries()
        kv_sib(1).wait_recv()

    loads[4].wait()
    pool_in[...] = jnp.dot(hidden[...], wpi[...], preferred_element_type=f32).astype(bf16)
    halo_next = remote(pool_in.at[pl.ds(TOK - 16, 16)], halo.at[pl.ds(0, 16)], halo_ss.at[0], halo_rs.at[0], next_dev)
    halo_prev = remote(pool_in.at[pl.ds(0, 16)], halo.at[pl.ds(16, 16)], halo_ss.at[1], halo_rs.at[1], prev_dev)
    halo_next.start()
    halo_prev.start()


    mine = pl.ds(c * HALF, HALF)
    loads[3].wait()
    key_pre = lax.dot_general(
        hidden[mine, :], wkr[...], (((1,), (1,)), ((), ())), preferred_element_type=f32
    )
    key_pre = jnp.concatenate([key_pre, key_pre], axis=1).astype(bf16).astype(f32)
    key_rope = turned(key_pre, cos_s[mine, :], sin_s[mine, :]).astype(bf16)

    @pl.when(c == 1)
    def _():
        kv_got("upf").wait_recv()
        kv_got("dnf").wait_recv()
        kv_sib(2).start()

    @pl.when(c == 0)
    def _():
        kv_sib(2).wait_recv()

    loads[14].wait()
    kv_pre = jnp.dot(hidden[mine, :], wkv[...], preferred_element_type=f32).astype(bf16)
    own0 = x * HALF
    own1 = SEQ // 2 + z * HALF
    own_rows = pl.ds(pl.multiple_of(jnp.where(c == 1, own0, own1), HALF), HALF)
    kv[own_rows, :KR] = scaled_rows(kv_pre.astype(f32), kv_gain_s[...], KR).astype(bf16)
    kv[own_rows, KR:] = key_rope

    def blk0(xx):
        return kv.at[pl.ds(xx * HALF, HALF)]

    def blk1(zz):
        return kv.at[pl.ds(SEQ // 2 + zz * HALF, HALF)]

    def first0(i):
        to = lax.rem(x + i, NX)
        return remote(blk0(x), blk0(x), p1_ss.at[i], p1_rs.at[i], {"sp_1": to})

    def first0_got(i):
        view = blk0(lax.rem(x + NX - i, NX))
        return remote(view, view, p1_ss.at[i], p1_rs.at[i], x_up)

    def first1(i):
        to = lax.rem(z + i, NZ)
        return remote(blk1(z), blk1(z), p1_ss.at[i], p1_rs.at[i], {"sp_0": to})

    def first1_far():
        view = blk1(lax.rem(z + 3, NZ))
        return remote(view, view, p1_ss.at[4], p1_rs.at[4], z_down)

    def first1_got(i):
        view = blk1(lax.rem(z + NZ - i, NZ))
        return remote(view, view, p1_ss.at[i], p1_rs.at[i], z_up)

    @pl.when(c == 1)
    def _():
        for i in (1, 3, 2):
            first0(i).start()

    @pl.when(c == 0)
    def _():
        for i in (1, 7, 2, 6, 5, 3):
            first1(i).start()

    q_got("up1").wait_recv()
    q_send("upf").start()
    q_got("dn1").wait_recv()
    q_send("dnf").start()

    def unit(cls, n):
        return kv.at[pl.ds(cls * (SEQ // 2) + n * UNIT, UNIT)]

    def half_unit(n, h):
        return kv.at[pl.ds(n * UNIT + h * (UNIT // 2), UNIT // 2)]

    def ring(src, dst, i, dev):
        return remote(src, dst, ring_ss.at[i], ring_rs.at[i], dev)

    def sends_after(cls, n):
        if cls == 0:
            up, down = z_up, z_down
            if n == 0:
                return [ring(unit(0, 0), unit(0, 1), 1, up), ring(unit(0, 0), unit(0, 2), 2, down)]
            if n < 5:
                return [ring(unit(0, n), unit(0, n + 2), n + 2, up if n % 2 else down)]
            if n < 7:
                return [ring(half_unit(n, n - 5), half_unit(7, n - 5), n + 2, up if n % 2 else down)]
            return []
        up, down = x_up, x_down
        if n == 0:
            return [
                ring(unit(1, 0), unit(1, 2), 2, up),
                ring(unit(1, 1), unit(1, 3), 3, down),
                ring(unit(1, 1), unit(1, 4), 4, up),
                ring(unit(1, 0), unit(1, 5), 5, down),
            ]
        if n == 2:
            return [ring(unit(1, 2), unit(1, 6), 6, up)]
        if n == 3:
            return [ring(unit(1, 3), unit(1, 7), 7, down)]
        return []

    def arrivals_for(cls, n):
        if cls == 0 and n == 7:
            return [ring(half_unit(7, h), half_unit(7, h), 7 + h, z_up) for h in range(2)]
        return [ring(unit(cls, n), unit(cls, n), n, z_up)]

    def sib(cls, n):
        return remote(unit(cls, n), unit(cls, n), sib_ss.at[n], sib_rs.at[n], other)

    def acquire_own(cls, n):
        for copy in arrivals_for(cls, n):
            copy.wait_recv()
        for copy in sends_after(cls, n):
            copy.start()
        sib(cls, n).start()

    @pl.when(c == 1)
    def _():
        for i in (1, 3, 2):
            first0_got(i).wait_recv()
        for copy in sends_after(0, 0):
            copy.start()
        sib(0, 0).start()


    q_got("up2").wait_recv()
    q_sib(0).start()
    q_got("dn2").wait_recv()
    q_sib(1).start()

    remote(halo.at[pl.ds(0, 16)], halo.at[pl.ds(0, 16)], halo_ss.at[0], halo_rs.at[0], next_dev).wait_recv()
    remote(halo.at[pl.ds(16, 16)], halo.at[pl.ds(16, 16)], halo_ss.at[1], halo_rs.at[1], next_dev).wait_recv()
    loads[6].wait()
    loads[7].wait()
    row_i = lax.broadcasted_iota(jnp.int32, (TOK, TOK), 0)
    gap = lax.broadcasted_iota(jnp.int32, (TOK, TOK), 1) - row_i
    rim_row = lax.broadcasted_iota(jnp.int32, (TOK, 32), 0)
    rim_col = lax.broadcasted_iota(jnp.int32, (TOK, 32), 1)
    before = rim_col < 16
    rim_gap = jnp.where(before, rim_col - 16, rim_col - 16 + TOK) - rim_row
    rim_ok = (before & (sp > 0)) | (~before & (sp < NZ * NX - 1))
    place = lax.broadcasted_iota(jnp.int32, (TOK, POOL_GROUP), 0) + sp * TOK
    for g in range(2):
        span = (1 + 3 * c) * (1 + g)
        cols = slice(g * POOL_GROUP, (g + 1) * POOL_GROUP)
        near = ((gap >= -span) & (gap < span)).astype(f32).astype(bf16)
        rim = ((rim_gap >= -span) & (rim_gap < span) & rim_ok).astype(f32).astype(bf16)
        sums = jnp.dot(near, pool_in[:, cols], preferred_element_type=f32)
        sums = sums + jnp.dot(rim, halo[:, cols], preferred_element_type=f32)
        low = jnp.maximum(place - span, 0)
        high = jnp.minimum(place + span, SEQ)
        mean = (sums / (high - low).astype(f32)).astype(bf16)
        spread = (mean.astype(f32) - pool_in[:, cols].astype(f32)).astype(bf16)
        pooled[:, cols] = jnp.dot(spread, mix[g], preferred_element_type=f32).astype(bf16)
    for j in range(4):
        cols = slice(j * 512, (j + 1) * 512)
        out_sum[:, cols] = jnp.dot(pooled[...], wop[:, cols], preferred_element_type=f32)

    @pl.when(c == 0)
    def _():
        first1_got(5).wait_recv()
        first1_far().start()

    def query_part(of):
        at = pl.ds(pl.multiple_of(of * 512, 512), 512)
        return jnp.dot(hidden[:, at], wq[at, :], preferred_element_type=f32)

    q_sib_got(0).wait_recv()
    q_sib_got(1).wait_recv()
    q_sum[...] = query_part(y) + query_part(y1) + query_part(y2)
    q_got("upf").wait_recv()
    q_got("dnf").wait_recv()
    q_sib(2).start()
    for i in (8, 9, 10, 13):
        loads[i].wait()
    @pl.when(c == 0)
    def _():
        for i in (1, 7, 2, 6, 3, 4):
            first1_got(i).wait_recv()
        for copy in sends_after(1, 0):
            copy.start()
        sib(1, 0).start()
        sib(1, 1).start()

    q_sib_got(2).wait_recv()
    q_pre = (q_sum[...] + query_part(y3)).astype(bf16)
    q_lat[...] = scaled_rows(q_pre.astype(f32), q_gain_s[...], QR).astype(bf16)
    q_nope[...] = jnp.dot(q_lat[...], wqn[...], preferred_element_type=f32).astype(bf16)
    q_rot = jnp.dot(q_lat[...], wqr[...], preferred_element_type=f32).astype(bf16).astype(f32)
    lane = lax.broadcasted_iota(jnp.int32, (TOK, 128), 1)
    for h in range(HEADS):
        rows = slice(h * TOK, (h + 1) * TOK)
        if h % 2 == 0:
            pair = turned(q_rot[:, h * 64 : h * 64 + 128], cos_s[...], sin_s[...]) * SCALE
        keep = lane < 64 if h % 2 == 0 else lane >= 64
        q_all[rows, KR:] = jnp.where(keep, pair, 0.0).astype(bf16)
        head = slice(h * NOPE_DIM, (h + 1) * NOPE_DIM)
        absorbed = lax.dot_general(
            q_nope[:, head], wku[:, head], (((1,), (1,)), ((), ())), preferred_element_type=f32
        )
        q_all[rows, :KR] = (absorbed * SCALE).astype(bf16)

    @pl.when(c == 1)
    def _():
        acquire_own(0, 1)

    steps = 2 * (SEQ // 2) // STEP

    def row_of(i):
        cls = lax.rem(i + 1 - c, 2)
        return pl.multiple_of(cls * (SEQ // 2) + (i // 2) * STEP, STEP)

    def acquire(i):
        @pl.when((i == 1) & (c == 1))
        def _():
            acquire_own(0, 2)

        for m in range(1, 4):

            @pl.when((i == 2 * m) & (c == 1))
            def _():
                for n in (2 * m + 1, 2 * m + 2):
                    if n < 8:
                        acquire_own(0, n)

            @pl.when((i == 2 * m) & (c == 0))
            def _():
                for n in (2 * m, 2 * m + 1):
                    acquire_own(1, n)

        @pl.when(lax.rem(i, 2) == 1)
        def _():
            for n in range(2):
                at = c * (SEQ // 2) + (i // 2) * STEP + n * UNIT
                view = kv.at[pl.ds(at, UNIT)]
                remote(view, view, sib_ss.at[i - 1 + n], sib_rs.at[i - 1 + n], other).wait_recv()

    def scores(i, h):
        s_scr[h % 2] = lax.dot_general(
            q_all[h * MB : (h + 1) * MB, :],
            kv[pl.ds(row_of(i), STEP), :],
            (((1,), (1,)), ((), ())),
            preferred_element_type=f32,
        )

    def softmax(h):
        for r in range(0, MB, SUB):
            g = slice(h * MB + r, h * MB + r + SUB)
            s = [s_scr[h % 2, r : r + SUB, j * 128 : (j + 1) * 128] for j in range(STEP // 128)]
            m_old = m_s[g, :]
            top = s[0]
            for t in s[1:]:
                top = jnp.maximum(top, t)
            m_new = jnp.maximum(m_old, jnp.max(top, axis=1, keepdims=True))
            alpha = jnp.exp2(m_old - m_new)
            total = l_s[g, :] * alpha
            for j, t in enumerate(s):
                p = jnp.exp2(t - m_new)
                total = total + p
                p_scr[h % 2, r : r + SUB, j * 128 : (j + 1) * 128] = p.astype(bf16)
            m_s[g, :] = m_new
            l_s[g, :] = total
            for j in range(2):
                cols = slice(j * 128, (j + 1) * 128)
                acc[g, cols] = acc[g, cols] * alpha

    def product(i, h):
        g = slice(h * MB, (h + 1) * MB)
        acc[g, :] = acc[g, :] + jnp.dot(p_scr[h % 2], kv[pl.ds(row_of(i), STEP), :KR], preferred_element_type=f32)

    chunks = ROWS // MB
    zero = jnp.int32(0)
    scores(zero, 0)
    for h in range(chunks - 1):
        scores(zero, h + 1)
        softmax(h)
        if h > 0:
            product(zero, h - 1)

    def step(i, carry):
        acquire(i + 1)
        scores(i + 1, 0)
        softmax(chunks - 1)
        product(i, chunks - 2)
        for h in range(chunks - 1):
            scores(i + 1, h + 1)
            softmax(h)
            if h == 0:
                product(i, chunks - 1)
            else:
                product(i + 1, h - 1)
        return carry

    lax.fori_loop(0, steps - 1, step, 0)
    end = jnp.int32(steps - 1)
    softmax(chunks - 1)
    product(end, chunks - 2)
    product(end, chunks - 1)

    loads[11].wait()
    loads[12].wait()
    for h in range(HEADS):
        rows = slice(h * TOK, (h + 1) * TOK)
        head = slice(h * VALUE_DIM, (h + 1) * VALUE_DIM)
        total = jnp.sum(l_s[rows, :], axis=1, keepdims=True)
        weighted = (acc[rows, :] / total).astype(bf16)
        att[:, head] = jnp.dot(weighted, wvu[:, head], preferred_element_type=f32).astype(bf16)

    theirs = pl.ds((1 - c) * HALF, HALF)

    def share(j):
        return remote(send_buf.at[j], recv_buf.at[j], out_ss.at[j], out_rs.at[j], other)

    def projected(rows, cols):
        return out_sum[rows, cols] + jnp.dot(att[rows, :], woa[:, cols], preferred_element_type=f32)

    blocks = [slice(j * 512, (j + 1) * 512) for j in range(4)]
    for j, cols in enumerate(blocks):
        send_buf[j] = projected(theirs, cols).astype(bf16)
        share(j).start()
    for cols in blocks:
        out_sum[mine, cols] = projected(mine, cols)
    for j, cols in enumerate(blocks):
        share(j).wait_recv()
        out[:, cols] = (out_sum[mine, cols] + recv_buf[j].astype(f32)).astype(bf16)

    tok_copy.wait_send()
    gain_copy.wait_send()
    for name in ("up1", "up2", "dn1", "dn2", "upf", "dnf"):
        q_send(name).wait_send()
    for i in range(3):
        q_sib(i).wait_send()
    halo_next.wait_send()
    halo_prev.wait_send()
    for j in range(4):
        share(j).wait_send()

    @pl.when(c == 1)
    def _():
        for name in ("up1", "up2", "dn1", "dn2", "upf", "dnf"):
            kv_send(name).wait_send()
        for i in range(3):
            kv_sib(i).wait_send()
        for i in range(1, NX):
            first0(i).wait_send()
        for n in range(8):
            for copy in sends_after(0, n):
                copy.wait_send()
            sib(0, n).wait_send()

    @pl.when(c == 0)
    def _():
        for i in (1, 2, 3, 5, 6, 7):
            first1(i).wait_send()
        first1_far().wait_send()
        for n in range(8):
            for copy in sends_after(1, n):
                copy.wait_send()
            sib(1, n).wait_send()


def on_device(
    tokens,
    norm_gain,
    w_q_down,
    q_gain,
    w_q_nope,
    w_q_rope,
    w_kv_down,
    kv_gain,
    w_k_up,
    w_v_up,
    w_k_rope,
    w_pool_in,
    w_pool_mix,
    w_out_attn,
    w_out_pool,
):
    row_table, col_table = rope_tables()
    anywhere = pl.BlockSpec(memory_space=pl.ANY)
    vmem = pl.BlockSpec(memory_space=pltpu.VMEM)
    dma = pltpu.SemaphoreType.DMA
    result = pl.pallas_call(
        layer_body,
        out_shape=jax.ShapeDtypeStruct((HALF, D), bf16),
        in_specs=[anywhere] * 17,
        out_specs=vmem,
        scratch_shapes=[
            pltpu.VMEM((2, TOK, 1024), bf16),
            pltpu.VMEM((2, 8, 128), bf16),
            pltpu.VMEM((1, QR), f32),
            pltpu.VMEM((1, KR), f32),
            pltpu.VMEM((2, SEQ // GRID_W, 128), f32),
            pltpu.VMEM((2, GRID_W, 128), f32),
            pltpu.VMEM((TOK, D), bf16),
            pltpu.VMEM((D, KR), bf16),
            pltpu.VMEM((D, QR), bf16),
            pltpu.VMEM((ROPE_DIM, D), bf16),
            pltpu.VMEM((D, 512), bf16),
            pltpu.VMEM((QR, 1024), bf16),
            pltpu.VMEM((QR, 512), bf16),
            pltpu.VMEM((KR, 1024), bf16),
            pltpu.VMEM((KR, 1024), bf16),
            pltpu.VMEM((2, POOL_GROUP, POOL_GROUP), bf16),
            pltpu.VMEM((1024, D), bf16),
            pltpu.VMEM((512, D), bf16),
            pltpu.VMEM((TOK, 128), f32),
            pltpu.VMEM((TOK, 128), f32),
            pltpu.VMEM((SEQ, WIDE), bf16),
            pltpu.VMEM((ROWS, WIDE), bf16),
            pltpu.VMEM((TOK, QR), f32),
            pltpu.VMEM((TOK, QR), bf16),
            pltpu.VMEM((TOK, 1024), bf16),
            pltpu.VMEM((TOK, 512), bf16),
            pltpu.VMEM((32, 512), bf16),
            pltpu.VMEM((TOK, 512), bf16),
            pltpu.VMEM((TOK, D), f32),
            pltpu.VMEM((TOK, 1024), bf16),
            pltpu.VMEM((4, HALF, 512), bf16),
            pltpu.VMEM((4, HALF, 512), bf16),
            pltpu.VMEM((2, MB, STEP), f32),
            pltpu.VMEM((2, MB, STEP), bf16),
            pltpu.VMEM((ROWS, KR), f32),
            pltpu.VMEM((ROWS, 128), f32),
            pltpu.VMEM((ROWS, 128), f32),
            dma((17,)),
            dma((2,)),
            dma((2,)),
            dma((2, 6)),
            dma((2, 6)),
            dma((2, 3)),
            dma((2, 3)),
            dma((8,)),
            dma((8,)),
            dma((9,)),
            dma((9,)),
            dma((8,)),
            dma((8,)),
            dma((2,)),
            dma((2,)),
            dma((4,)),
            dma((4,)),
        ],
        compiler_params=pltpu.CompilerParams(
            collective_id=0, has_side_effects=True, vmem_limit_bytes=60 * 2**20
        ),
    )(
        tokens[0],
        norm_gain.reshape(8, 128),
        w_q_down,
        q_gain[None],
        w_q_nope,
        w_q_rope,
        w_kv_down,
        kv_gain[None],
        w_k_up,
        w_v_up,
        w_k_rope.T,
        w_pool_in,
        w_pool_mix,
        w_out_attn,
        w_out_pool,
        jnp.asarray(row_table),
        jnp.asarray(col_table),
    )
    return result[None]


def solution(mesh):
    torus = Mesh(
        mesh.devices.reshape(NZ, NX, mesh.shape["fs"], mesh.shape["tp"]), ("sp_0", "sp_1", "fs", "tp")
    )
    placed = (
        P("fs", SP, "tp"),
        P("tp"),
        P("fs", None),
        P(),
        P(None, "tp"),
        P(None, "tp"),
        P("fs", None),
        P(),
        P(None, "tp"),
        P(None, "tp"),
        P(),
        P(None, "tp"),
        P(),
        P("tp", None),
        P("tp", None),
    )
    return jax.shard_map(
        on_device, mesh=torus, in_specs=placed, out_specs=P("fs", SP_TP, None), check_vma=False
    )
```

```python
import functools

import jax
import jax.numpy as jnp
import numpy as np
from jax import lax
from jax.experimental import pallas as pl
from jax.experimental.pallas import tpu as pltpu
from jax.sharding import Mesh
from jax.sharding import PartitionSpec as P

NOPE_DIM = 128
ROPE_DIM = 64
VALUE_DIM = 128
GRID_W = 64
POOL_GROUP = 256
SP = ("sp_0", "sp_1")
SP_TP = ("sp_0", "sp_1", "tp")
EPS = 1e-06
THETA = 10000.0
LOG2E = 1.4426950408889634
MESH = pl.DeviceIdType.MESH

NZ, NX, NY = 8, 4, 4
TOK = 192
HALF = 96
D = 2048
HEADS = 8
QR, KR = 512, 256
WIDE = 384
UNIT = 384
ROWS = HEADS * TOK
MB = 256
STEP = 2 * UNIT
SUB = 32
SEQ = NZ * NX * TOK
SCALE = (NOPE_DIM + ROPE_DIM) ** (-0.5) * LOG2E
f32, bf16 = jnp.float32, jnp.bfloat16


def rope_tables():
    inverse = (THETA ** (-np.arange(0, ROPE_DIM // 2, 2) / (ROPE_DIM // 2))).astype(np.float32)
    lane = np.arange(128)
    freq = inverse[lane % 16]
    by_row = (lane // 32) % 2 == 0
    sign = np.where((lane // 16) % 2 == 0, -1.0, 1.0)

    def table(count, keep):
        angle = (np.arange(count, dtype=np.float32)[:, None] * freq).astype(np.float64)
        cos = np.where(keep, np.cos(angle), 0.0)
        sin = np.where(keep, np.sin(angle) * sign, 0.0)
        return np.stack([cos, sin]).astype(np.float32)

    return table(SEQ // GRID_W, by_row), table(GRID_W, ~by_row)


def turned(values, cos, sin):
    lane = lax.broadcasted_iota(jnp.int32, values.shape, 1)
    ahead = pltpu.roll(values, 112, 1)
    behind = pltpu.roll(values, 16, 1)
    partner = jnp.where((lane // 16) % 2 == 0, ahead, behind)
    return values * cos + partner * sin


def scaled_rows(values, gain, width):
    mean = jnp.sum(values * values, axis=1, keepdims=True) * (1.0 / width)
    return values * lax.rsqrt(mean + EPS) * gain


def layer_body(
    tokens,
    norm_gain,
    w_q_down,
    q_gain,
    w_q_nope,
    w_q_rope,
    w_kv_down,
    kv_gain,
    w_k_up,
    w_v_up,
    w_k_rope,
    w_pool_in,
    w_pool_mix,
    w_out_attn,
    w_out_pool,
    row_hbm,
    col_hbm,
    out,
    tok,
    gains,
    q_gain_s,
    kv_gain_s,
    row_table,
    col_table,
    hidden,
    wkv,
    wq,
    wkr,
    wpi,
    wqn,
    wqr,
    wku,
    wvu,
    mix,
    woa,
    wop,
    cos_s,
    sin_s,
    kv,
    q_all,
    q_sum,
    q_lat,
    q_nope,
    pool_in,
    halo,
    pooled,
    out_sum,
    att,
    send_buf,
    recv_buf,
    s_scr,
    p_scr,
    acc,
    m_s,
    l_s,
    loc,
    tok_ss,
    tok_rs,
    w_ss,
    w_rs,
    ws_ss,
    ws_rs,
    p1_ss,
    p1_rs,
    ring_ss,
    ring_rs,
    sib_ss,
    sib_rs,
    halo_ss,
    halo_rs,
    out_ss,
    out_rs,
):
    z, x = lax.axis_index("sp_0"), lax.axis_index("sp_1")
    y, c = lax.axis_index("fs"), lax.axis_index("tp")
    sp = z * NX + x
    other = {"tp": 1 - c}
    y_up, y_down = {"fs": lax.rem(y + 1, NY)}, {"fs": lax.rem(y + NY - 1, NY)}
    z_up, z_down = {"sp_0": lax.rem(z + 1, NZ)}, {"sp_0": lax.rem(z + NZ - 1, NZ)}
    x_up, x_down = {"sp_1": lax.rem(x + 1, NX)}, {"sp_1": lax.rem(x + NX - 1, NX)}
    sp_next, sp_prev = lax.rem(sp + 1, NZ * NX), lax.rem(sp + NZ * NX - 1, NZ * NX)
    next_dev = {"sp_0": sp_next // NX, "sp_1": sp_next % NX}
    prev_dev = {"sp_0": sp_prev // NX, "sp_1": sp_prev % NX}

    def remote(src, dst, ssem, rsem, dev):
        return pltpu.make_async_remote_copy(
            src_ref=src, dst_ref=dst, send_sem=ssem, recv_sem=rsem, device_id=dev, device_id_type=MESH
        )

    barrier = pltpu.get_barrier_semaphore()
    partners = [other, y_up, y_down, next_dev, prev_dev]
    partners += [{"sp_0": lax.rem(z + i, NZ)} for i in range(1, NZ)]
    partners += [{"sp_1": lax.rem(x + i, NX)} for i in range(1, NX)]
    for dev in partners:
        pl.semaphore_signal(barrier, inc=1, device_id=dev, device_id_type=MESH)

    def local(i, src, dst):
        return pltpu.make_async_copy(src, dst, loc.at[i])

    loads = [
        local(0, tokens, tok.at[c]),
        local(1, norm_gain, gains.at[c]),
        local(2, w_kv_down, wkv.at[pl.ds(y * 512, 512)]),
        local(3, w_k_rope, wkr),
        local(4, w_pool_in, wpi),
        local(5, w_q_down, wq.at[pl.ds(y * 512, 512)]),
        local(6, w_pool_mix.at[pl.ds(2 * c, 2)], mix),
        local(7, w_out_pool, wop),
        local(8, w_q_nope, wqn),
        local(9, w_q_rope, wqr),
        local(10, w_k_up, wku),
        local(11, w_v_up, wvu),
        local(12, w_out_attn, woa),
        local(13, q_gain, q_gain_s),
        local(14, kv_gain, kv_gain_s),
        local(15, row_hbm, row_table),
        local(16, col_hbm, col_table),
    ]
    for i in (0, 1, 2, 15, 16, 5):
        loads[i].start()

    m_s[...] = jnp.full(m_s.shape, -1e30, f32)
    l_s[...] = jnp.zeros(l_s.shape, f32)
    acc[...] = jnp.zeros(acc.shape, f32)
    pl.semaphore_wait(barrier, len(partners))

    tok_copy = remote(tok.at[c], tok.at[c], tok_ss.at[0], tok_rs.at[0], other)
    gain_copy = remote(gains.at[c], gains.at[c], tok_ss.at[1], tok_rs.at[1], other)
    loads[0].wait()
    loads[1].wait()
    tok_copy.start()
    gain_copy.start()

    y1, y2, y3 = lax.rem(y + 3, NY), lax.rem(y + 1, NY), lax.rem(y + 2, NY)

    def weight_copies(w, buf, base, part):
        def rows(of, p):
            return buf.at[pl.ds(of * 512 + base + p * part, part)]

        ss, rs = w_ss.at[w], w_rs.at[w]

        def copy(i, of, p, dev):
            return remote(rows(of, p), rows(of, p), ss.at[i], rs.at[i], dev)

        def sends(name):
            return {
                "up1": lambda: copy(0, y, 0, y_up),
                "up2": lambda: copy(1, y, 1, y_up),
                "dn1": lambda: copy(2, y, 1, y_down),
                "dn2": lambda: copy(3, y, 0, y_down),
                "upf": lambda: copy(4, y1, 0, y_up),
                "dnf": lambda: copy(5, y2, 1, y_down),
            }[name]()

        def got(name):
            return {
                "up1": lambda: copy(0, y1, 0, y_up),
                "up2": lambda: copy(1, y1, 1, y_up),
                "dn1": lambda: copy(2, y2, 1, y_up),
                "dn2": lambda: copy(3, y2, 0, y_up),
                "upf": lambda: copy(4, y3, 0, y_up),
                "dnf": lambda: copy(5, y3, 1, y_up),
            }[name]()

        return sends, got

    def weight_sibling(w, buf, base, count, i):
        view = buf.at[pl.ds((y1, y2, y3)[i] * 512 + base, count)]
        return remote(view, view, ws_ss.at[w, i], ws_rs.at[w, i], other)

    kv_send, kv_got = weight_copies(0, wkv, 0, 256)
    q_send, q_got = weight_copies(1, wq, c * 256, 128)

    def kv_sib(i):
        return weight_sibling(0, wkv, 0, 512, i)

    def q_sib(i):
        return weight_sibling(1, wq, c * 256, 256, i)

    def q_sib_got(i):
        return weight_sibling(1, wq, (1 - c) * 256, 256, i)

    def start_queries():
        for name in ("up1", "dn1", "up2", "dn2"):
            q_send(name).start()

    loads[2].wait()

    @pl.when(c == 1)
    def _():
        for name in ("up1", "dn1", "up2", "dn2"):
            kv_send(name).start()

    for i in (3, 4, 6, 7, 8, 9, 10, 11, 13, 14, 12):
        loads[i].start()
    loads[5].wait()

    loads[15].wait()
    loads[16].wait()
    for k in range(TOK // GRID_W):
        rows = slice(k * GRID_W, (k + 1) * GRID_W)
        at = 3 * sp + k
        cos_s[rows, :] = row_table[0, pl.ds(at, 1), :] + col_table[0]
        sin_s[rows, :] = row_table[1, pl.ds(at, 1), :] + col_table[1]

    remote(tok.at[1 - c], tok.at[1 - c], tok_ss.at[0], tok_rs.at[0], other).wait_recv()
    remote(gains.at[1 - c], gains.at[1 - c], tok_ss.at[1], tok_rs.at[1], other).wait_recv()
    gain = [gains[half].astype(f32) for half in range(2)]
    for r in range(0, TOK, 16):
        parts = [tok[half, r : r + 16, :].astype(f32) for half in range(2)]
        total = jnp.sum(parts[0] * parts[0] + parts[1] * parts[1], axis=1, keepdims=True)
        inv = lax.rsqrt(total * (1.0 / D) + EPS)
        for half in range(2):
            for j in range(8):
                cols = slice(j * 128, (j + 1) * 128)
                at = half * 1024 + j * 128
                hidden[r : r + 16, at : at + 128] = (parts[half][:, cols] * inv * gain[half][j : j + 1, :]).astype(bf16)
    @pl.when(c == 1)
    def _():
        kv_got("up1").wait_recv()
        kv_send("upf").start()
        kv_got("dn1").wait_recv()
        kv_send("dnf").start()
        start_queries()
        kv_got("up2").wait_recv()
        kv_sib(0).start()
        kv_got("dn2").wait_recv()
        kv_sib(1).start()

    @pl.when(c == 0)
    def _():
        kv_sib(0).wait_recv()
        start_queries()
        kv_sib(1).wait_recv()

    loads[4].wait()
    pool_in[...] = jnp.dot(hidden[...], wpi[...], preferred_element_type=f32).astype(bf16)
    halo_next = remote(pool_in.at[pl.ds(TOK - 16, 16)], halo.at[pl.ds(0, 16)], halo_ss.at[0], halo_rs.at[0], next_dev)
    halo_prev = remote(pool_in.at[pl.ds(0, 16)], halo.at[pl.ds(16, 16)], halo_ss.at[1], halo_rs.at[1], prev_dev)
    halo_next.start()
    halo_prev.start()


    mine = pl.ds(c * HALF, HALF)
    loads[3].wait()
    key_pre = lax.dot_general(
        hidden[mine, :], wkr[...], (((1,), (1,)), ((), ())), preferred_element_type=f32
    )
    key_pre = jnp.concatenate([key_pre, key_pre], axis=1).astype(bf16).astype(f32)
    key_rope = turned(key_pre, cos_s[mine, :], sin_s[mine, :]).astype(bf16)

    @pl.when(c == 1)
    def _():
        kv_got("upf").wait_recv()
        kv_got("dnf").wait_recv()
        kv_sib(2).start()

    @pl.when(c == 0)
    def _():
        kv_sib(2).wait_recv()

    loads[14].wait()
    kv_pre = jnp.dot(hidden[mine, :], wkv[...], preferred_element_type=f32).astype(bf16)
    own0 = x * HALF
    own1 = SEQ // 2 + z * HALF
    own_rows = pl.ds(pl.multiple_of(jnp.where(c == 1, own0, own1), HALF), HALF)
    kv[own_rows, :KR] = scaled_rows(kv_pre.astype(f32), kv_gain_s[...], KR).astype(bf16)
    kv[own_rows, KR:] = key_rope

    def blk0(xx):
        return kv.at[pl.ds(xx * HALF, HALF)]

    def blk1(zz):
        return kv.at[pl.ds(SEQ // 2 + zz * HALF, HALF)]

    def first0(i):
        to = lax.rem(x + i, NX)
        return remote(blk0(x), blk0(x), p1_ss.at[i], p1_rs.at[i], {"sp_1": to})

    def first0_got(i):
        view = blk0(lax.rem(x + NX - i, NX))
        return remote(view, view, p1_ss.at[i], p1_rs.at[i], x_up)

    def first1(i):
        to = lax.rem(z + i, NZ)
        return remote(blk1(z), blk1(z), p1_ss.at[i], p1_rs.at[i], {"sp_0": to})

    def first1_far():
        view = blk1(lax.rem(z + 3, NZ))
        return remote(view, view, p1_ss.at[4], p1_rs.at[4], z_down)

    def first1_got(i):
        view = blk1(lax.rem(z + NZ - i, NZ))
        return remote(view, view, p1_ss.at[i], p1_rs.at[i], z_up)

    @pl.when(c == 1)
    def _():
        for i in (1, 3, 2):
            first0(i).start()

    @pl.when(c == 0)
    def _():
        for i in (1, 7, 2, 6, 5, 3):
            first1(i).start()

    q_got("up1").wait_recv()
    q_send("upf").start()
    q_got("dn1").wait_recv()
    q_send("dnf").start()

    def unit(cls, n):
        return kv.at[pl.ds(cls * (SEQ // 2) + n * UNIT, UNIT)]

    def half_unit(n, h):
        return kv.at[pl.ds(n * UNIT + h * (UNIT // 2), UNIT // 2)]

    def ring(src, dst, i, dev):
        return remote(src, dst, ring_ss.at[i], ring_rs.at[i], dev)

    def sends_after(cls, n):
        if cls == 0:
            up, down = z_up, z_down
            if n == 0:
                return [ring(unit(0, 0), unit(0, 1), 1, up), ring(unit(0, 0), unit(0, 2), 2, down)]
            if n < 5:
                return [ring(unit(0, n), unit(0, n + 2), n + 2, up if n % 2 else down)]
            if n < 7:
                return [ring(half_unit(n, n - 5), half_unit(7, n - 5), n + 2, up if n % 2 else down)]
            return []
        up, down = x_up, x_down
        if n == 0:
            return [
                ring(unit(1, 0), unit(1, 2), 2, up),
                ring(unit(1, 1), unit(1, 3), 3, down),
                ring(unit(1, 1), unit(1, 4), 4, up),
                ring(unit(1, 0), unit(1, 5), 5, down),
            ]
        if n == 2:
            return [ring(unit(1, 2), unit(1, 6), 6, up)]
        if n == 3:
            return [ring(unit(1, 3), unit(1, 7), 7, down)]
        return []

    def arrivals_for(cls, n):
        if cls == 0 and n == 7:
            return [ring(half_unit(7, h), half_unit(7, h), 7 + h, z_up) for h in range(2)]
        return [ring(unit(cls, n), unit(cls, n), n, z_up)]

    def sib(cls, n):
        return remote(unit(cls, n), unit(cls, n), sib_ss.at[n], sib_rs.at[n], other)

    def acquire_own(cls, n):
        for copy in arrivals_for(cls, n):
            copy.wait_recv()
        for copy in sends_after(cls, n):
            copy.start()
        sib(cls, n).start()

    @pl.when(c == 1)
    def _():
        for i in (1, 3, 2):
            first0_got(i).wait_recv()
        for copy in sends_after(0, 0):
            copy.start()
        sib(0, 0).start()


    q_got("up2").wait_recv()
    q_sib(0).start()
    q_got("dn2").wait_recv()
    q_sib(1).start()

    remote(halo.at[pl.ds(0, 16)], halo.at[pl.ds(0, 16)], halo_ss.at[0], halo_rs.at[0], next_dev).wait_recv()
    remote(halo.at[pl.ds(16, 16)], halo.at[pl.ds(16, 16)], halo_ss.at[1], halo_rs.at[1], next_dev).wait_recv()
    loads[6].wait()
    loads[7].wait()
    row_i = lax.broadcasted_iota(jnp.int32, (TOK, TOK), 0)
    gap = lax.broadcasted_iota(jnp.int32, (TOK, TOK), 1) - row_i
    rim_row = lax.broadcasted_iota(jnp.int32, (TOK, 32), 0)
    rim_col = lax.broadcasted_iota(jnp.int32, (TOK, 32), 1)
    before = rim_col < 16
    rim_gap = jnp.where(before, rim_col - 16, rim_col - 16 + TOK) - rim_row
    rim_ok = (before & (sp > 0)) | (~before & (sp < NZ * NX - 1))
    place = lax.broadcasted_iota(jnp.int32, (TOK, POOL_GROUP), 0) + sp * TOK
    for g in range(2):
        span = (1 + 3 * c) * (1 + g)
        cols = slice(g * POOL_GROUP, (g + 1) * POOL_GROUP)
        near = ((gap >= -span) & (gap < span)).astype(f32).astype(bf16)
        rim = ((rim_gap >= -span) & (rim_gap < span) & rim_ok).astype(f32).astype(bf16)
        sums = jnp.dot(near, pool_in[:, cols], preferred_element_type=f32)
        sums = sums + jnp.dot(rim, halo[:, cols], preferred_element_type=f32)
        low = jnp.maximum(place - span, 0)
        high = jnp.minimum(place + span, SEQ)
        mean = (sums / (high - low).astype(f32)).astype(bf16)
        spread = (mean.astype(f32) - pool_in[:, cols].astype(f32)).astype(bf16)
        pooled[:, cols] = jnp.dot(spread, mix[g], preferred_element_type=f32).astype(bf16)
    for j in range(4):
        cols = slice(j * 512, (j + 1) * 512)
        out_sum[:, cols] = jnp.dot(pooled[...], wop[:, cols], preferred_element_type=f32)

    @pl.when(c == 0)
    def _():
        first1_got(5).wait_recv()
        first1_far().start()

    def query_part(of):
        at = pl.ds(pl.multiple_of(of * 512, 512), 512)
        return jnp.dot(hidden[:, at], wq[at, :], preferred_element_type=f32)

    q_sib_got(0).wait_recv()
    q_sib_got(1).wait_recv()
    q_sum[...] = query_part(y) + query_part(y1) + query_part(y2)
    q_got("upf").wait_recv()
    q_got("dnf").wait_recv()
    q_sib(2).start()
    for i in (8, 9, 10, 13):
        loads[i].wait()
    @pl.when(c == 0)
    def _():
        for i in (1, 7, 2, 6, 3, 4):
            first1_got(i).wait_recv()
        for copy in sends_after(1, 0):
            copy.start()
        sib(1, 0).start()
        sib(1, 1).start()

    q_sib_got(2).wait_recv()
    q_pre = (q_sum[...] + query_part(y3)).astype(bf16)
    q_lat[...] = scaled_rows(q_pre.astype(f32), q_gain_s[...], QR).astype(bf16)
    q_nope[...] = jnp.dot(q_lat[...], wqn[...], preferred_element_type=f32).astype(bf16)
    q_rot = jnp.dot(q_lat[...], wqr[...], preferred_element_type=f32).astype(bf16).astype(f32)
    lane = lax.broadcasted_iota(jnp.int32, (TOK, 128), 1)
    for h in range(HEADS):
        rows = slice(h * TOK, (h + 1) * TOK)
        if h % 2 == 0:
            pair = turned(q_rot[:, h * 64 : h * 64 + 128], cos_s[...], sin_s[...]) * SCALE
        keep = lane < 64 if h % 2 == 0 else lane >= 64
        q_all[rows, KR:] = jnp.where(keep, pair, 0.0).astype(bf16)
        head = slice(h * NOPE_DIM, (h + 1) * NOPE_DIM)
        absorbed = lax.dot_general(
            q_nope[:, head], wku[:, head], (((1,), (1,)), ((), ())), preferred_element_type=f32
        )
        q_all[rows, :KR] = (absorbed * SCALE).astype(bf16)

    @pl.when(c == 1)
    def _():
        acquire_own(0, 1)

    steps = 2 * (SEQ // 2) // STEP

    def row_of(i):
        cls = lax.rem(i + 1 - c, 2)
        return pl.multiple_of(cls * (SEQ // 2) + (i // 2) * STEP, STEP)

    def acquire(i):
        for n in range(2, 8):

            @pl.when((i == n - 1) & (c == 1))
            def _():
                acquire_own(0, n)

        for m in range(1, 4):

            @pl.when((i == 2 * m) & (c == 0))
            def _():
                for n in (2 * m, 2 * m + 1):
                    acquire_own(1, n)

        @pl.when(lax.rem(i, 2) == 1)
        def _():
            for n in range(2):
                at = c * (SEQ // 2) + (i // 2) * STEP + n * UNIT
                view = kv.at[pl.ds(at, UNIT)]
                remote(view, view, sib_ss.at[i - 1 + n], sib_rs.at[i - 1 + n], other).wait_recv()

    def scores(i, h):
        s_scr[h % 2] = lax.dot_general(
            q_all[h * MB : (h + 1) * MB, :],
            kv[pl.ds(row_of(i), STEP), :],
            (((1,), (1,)), ((), ())),
            preferred_element_type=f32,
        )

    def softmax(h):
        for r in range(0, MB, SUB):
            g = slice(h * MB + r, h * MB + r + SUB)
            s = [s_scr[h % 2, r : r + SUB, j * 128 : (j + 1) * 128] for j in range(STEP // 128)]
            m_old = m_s[g, :]
            top = s[0]
            for t in s[1:]:
                top = jnp.maximum(top, t)
            m_new = jnp.maximum(m_old, jnp.max(top, axis=1, keepdims=True))
            alpha = jnp.exp2(m_old - m_new)
            total = l_s[g, :] * alpha
            for j, t in enumerate(s):
                p = jnp.exp2(t - m_new)
                total = total + p
                p_scr[h % 2, r : r + SUB, j * 128 : (j + 1) * 128] = p.astype(bf16)
            m_s[g, :] = m_new
            l_s[g, :] = total
            for j in range(2):
                cols = slice(j * 128, (j + 1) * 128)
                acc[g, cols] = acc[g, cols] * alpha

    def product(i, h):
        g = slice(h * MB, (h + 1) * MB)
        acc[g, :] = acc[g, :] + jnp.dot(p_scr[h % 2], kv[pl.ds(row_of(i), STEP), :KR], preferred_element_type=f32)

    chunks = ROWS // MB
    zero = jnp.int32(0)
    scores(zero, 0)
    for h in range(chunks - 1):
        scores(zero, h + 1)
        softmax(h)
        if h > 0:
            product(zero, h - 1)

    def step(i, carry):
        acquire(i + 1)
        scores(i + 1, 0)
        softmax(chunks - 1)
        product(i, chunks - 2)
        for h in range(chunks - 1):
            scores(i + 1, h + 1)
            softmax(h)
            if h == 0:
                product(i, chunks - 1)
            else:
                product(i + 1, h - 1)
        return carry

    lax.fori_loop(0, steps - 1, step, 0)
    end = jnp.int32(steps - 1)
    softmax(chunks - 1)
    product(end, chunks - 2)
    product(end, chunks - 1)

    loads[11].wait()
    loads[12].wait()
    for h in range(HEADS):
        rows = slice(h * TOK, (h + 1) * TOK)
        head = slice(h * VALUE_DIM, (h + 1) * VALUE_DIM)
        total = jnp.sum(l_s[rows, :], axis=1, keepdims=True)
        weighted = (acc[rows, :] / total).astype(bf16)
        att[:, head] = jnp.dot(weighted, wvu[:, head], preferred_element_type=f32).astype(bf16)

    theirs = pl.ds((1 - c) * HALF, HALF)

    def share(j):
        return remote(send_buf.at[j], recv_buf.at[j], out_ss.at[j], out_rs.at[j], other)

    def projected(rows, cols):
        return out_sum[rows, cols] + jnp.dot(att[rows, :], woa[:, cols], preferred_element_type=f32)

    blocks = [slice(j * 512, (j + 1) * 512) for j in range(4)]
    for j, cols in enumerate(blocks):
        send_buf[j] = projected(theirs, cols).astype(bf16)
        share(j).start()
    for cols in blocks:
        out_sum[mine, cols] = projected(mine, cols)
    for j, cols in enumerate(blocks):
        share(j).wait_recv()
        out[:, cols] = (out_sum[mine, cols] + recv_buf[j].astype(f32)).astype(bf16)

    tok_copy.wait_send()
    gain_copy.wait_send()
    for name in ("up1", "up2", "dn1", "dn2", "upf", "dnf"):
        q_send(name).wait_send()
    for i in range(3):
        q_sib(i).wait_send()
    halo_next.wait_send()
    halo_prev.wait_send()
    for j in range(4):
        share(j).wait_send()

    @pl.when(c == 1)
    def _():
        for name in ("up1", "up2", "dn1", "dn2", "upf", "dnf"):
            kv_send(name).wait_send()
        for i in range(3):
            kv_sib(i).wait_send()
        for i in range(1, NX):
            first0(i).wait_send()
        for n in range(8):
            for copy in sends_after(0, n):
                copy.wait_send()
            sib(0, n).wait_send()

    @pl.when(c == 0)
    def _():
        for i in (1, 2, 3, 5, 6, 7):
            first1(i).wait_send()
        first1_far().wait_send()
        for n in range(8):
            for copy in sends_after(1, n):
                copy.wait_send()
            sib(1, n).wait_send()


def on_device(
    tokens,
    norm_gain,
    w_q_down,
    q_gain,
    w_q_nope,
    w_q_rope,
    w_kv_down,
    kv_gain,
    w_k_up,
    w_v_up,
    w_k_rope,
    w_pool_in,
    w_pool_mix,
    w_out_attn,
    w_out_pool,
):
    row_table, col_table = rope_tables()
    anywhere = pl.BlockSpec(memory_space=pl.ANY)
    vmem = pl.BlockSpec(memory_space=pltpu.VMEM)
    dma = pltpu.SemaphoreType.DMA
    result = pl.pallas_call(
        layer_body,
        out_shape=jax.ShapeDtypeStruct((HALF, D), bf16),
        in_specs=[anywhere] * 17,
        out_specs=vmem,
        scratch_shapes=[
            pltpu.VMEM((2, TOK, 1024), bf16),
            pltpu.VMEM((2, 8, 128), bf16),
            pltpu.VMEM((1, QR), f32),
            pltpu.VMEM((1, KR), f32),
            pltpu.VMEM((2, SEQ // GRID_W, 128), f32),
            pltpu.VMEM((2, GRID_W, 128), f32),
            pltpu.VMEM((TOK, D), bf16),
            pltpu.VMEM((D, KR), bf16),
            pltpu.VMEM((D, QR), bf16),
            pltpu.VMEM((ROPE_DIM, D), bf16),
            pltpu.VMEM((D, 512), bf16),
            pltpu.VMEM((QR, 1024), bf16),
            pltpu.VMEM((QR, 512), bf16),
            pltpu.VMEM((KR, 1024), bf16),
            pltpu.VMEM((KR, 1024), bf16),
            pltpu.VMEM((2, POOL_GROUP, POOL_GROUP), bf16),
            pltpu.VMEM((1024, D), bf16),
            pltpu.VMEM((512, D), bf16),
            pltpu.VMEM((TOK, 128), f32),
            pltpu.VMEM((TOK, 128), f32),
            pltpu.VMEM((SEQ, WIDE), bf16),
            pltpu.VMEM((ROWS, WIDE), bf16),
            pltpu.VMEM((TOK, QR), f32),
            pltpu.VMEM((TOK, QR), bf16),
            pltpu.VMEM((TOK, 1024), bf16),
            pltpu.VMEM((TOK, 512), bf16),
            pltpu.VMEM((32, 512), bf16),
            pltpu.VMEM((TOK, 512), bf16),
            pltpu.VMEM((TOK, D), f32),
            pltpu.VMEM((TOK, 1024), bf16),
            pltpu.VMEM((4, HALF, 512), bf16),
            pltpu.VMEM((4, HALF, 512), bf16),
            pltpu.VMEM((2, MB, STEP), f32),
            pltpu.VMEM((2, MB, STEP), bf16),
            pltpu.VMEM((ROWS, KR), f32),
            pltpu.VMEM((ROWS, 128), f32),
            pltpu.VMEM((ROWS, 128), f32),
            dma((17,)),
            dma((2,)),
            dma((2,)),
            dma((2, 6)),
            dma((2, 6)),
            dma((2, 3)),
            dma((2, 3)),
            dma((8,)),
            dma((8,)),
            dma((9,)),
            dma((9,)),
            dma((8,)),
            dma((8,)),
            dma((2,)),
            dma((2,)),
            dma((4,)),
            dma((4,)),
        ],
        compiler_params=pltpu.CompilerParams(
            collective_id=0, has_side_effects=True, vmem_limit_bytes=60 * 2**20
        ),
    )(
        tokens[0],
        norm_gain.reshape(8, 128),
        w_q_down,
        q_gain[None],
        w_q_nope,
        w_q_rope,
        w_kv_down,
        kv_gain[None],
        w_k_up,
        w_v_up,
        w_k_rope.T,
        w_pool_in,
        w_pool_mix,
        w_out_attn,
        w_out_pool,
        jnp.asarray(row_table),
        jnp.asarray(col_table),
    )
    return result[None]


def solution(mesh):
    torus = Mesh(
        mesh.devices.reshape(NZ, NX, mesh.shape["fs"], mesh.shape["tp"]), ("sp_0", "sp_1", "fs", "tp")
    )
    placed = (
        P("fs", SP, "tp"),
        P("tp"),
        P("fs", None),
        P(),
        P(None, "tp"),
        P(None, "tp"),
        P("fs", None),
        P(),
        P(None, "tp"),
        P(None, "tp"),
        P(),
        P(None, "tp"),
        P(),
        P("tp", None),
        P("tp", None),
    )
    return jax.shard_map(
        on_device, mesh=torus, in_specs=placed, out_specs=P("fs", SP_TP, None), check_vma=False
    )
```
